256 devices in a mesh: dp: 4 (over x), kv: 32 (over z, y), tp: 2 (over core).
Axes of the slice: x: 4, y: 4, z: 8, core: 2. Of those that a mesh axis runs over, the one named last changes fastest.
Arguments:
- tokens: bfloat16 [4, 16384, 2048], P('dp', 'kv'), may hold values from -6 to 6
- w_query: bfloat16 [2048, 1024], P(None, 'tp'), as said below
- w_key: bfloat16 [2048, 1024], P(None, 'tp'), as said below
- w_value: bfloat16 [2048, 1024], P(None, 'tp'), may hold values from -0.125 to 0.125
- w_out: bfloat16 [1024, 2048], P('tp'), may hold values from -0.1875 to 0.1875
- chosen: int32 [4, 256, 16], P('dp', 'kv'), may hold values from -1 to 255, as said below
Outputs:
- mixed: bfloat16 [4, 16384, 2048], P('dp', ('kv', 'tp'))
- log_sums: float32 [4, 16, 16384], P('dp', 'tp', 'kv')
The draws below stay inside these ranges and needn't reach their ends.
Inputs may be any that keep to these rules, and one draw needn't show every extreme that they name: `chosen`: write d = b // 8 and j = b % 8 for query block b. Row b lists b first, then min(15, j + 2 * d) distinct earlier blocks, then -1. Of the blocks that the query blocks of one index d of kv list, at most 2 lie in the positions of any one other index; the first query block of every index d >= 1 lists 2 blocks of index d - 1, and, where it exists, 2 blocks of the index half the sequence earlier. `w_query`: A weight matrix with entries up to about 4. `w_key`: A weight matrix of entries of order 2048 to the power -1/2.
All inputs are finite; a program needn't handle non-finite values.
Results may differ from the reference program's by a relative error of at most 0.0093.
Values may be sent and summed in bfloat16 or wider, within the bound.
A program may use at most 192 MiB of HBM per device.

```python
import jax
import jax.numpy as jnp
from jax import lax

D = 2048
HEADS = 16
HEAD_DIM = 64
BLOCK = 64
NSEL = 16
SEQS = 4
LENGTH = 16384
NBLK = 256
KB_DEV = 8
CAP = 2
N_TP = 2


def paired_weights(key):
    base = jax.random.fold_in(key, 11)
    scale = D ** (-0.5)
    key_weight = jnp.clip(jax.random.normal(jax.random.fold_in(base, 1), (D, HEADS * HEAD_DIM), jnp.float32), -6.0, 6.0) * scale
    free_weight = jnp.clip(jax.random.normal(jax.random.fold_in(base, 2), (D, HEADS * HEAD_DIM), jnp.float32), -6.0, 6.0) * scale
    query_weight = free_weight
    return (query_weight, key_weight)


def draw_w_query(key, part):
    return paired_weights(key)[0].astype(jnp.bfloat16)


def draw_w_key(key, part):
    return paired_weights(key)[1].astype(jnp.bfloat16)


def one_sequence(key):
    blocks = jnp.arange(NBLK, dtype=jnp.int32)
    owners = blocks // KB_DEV
    within = blocks % KB_DEV
    devices = NBLK // KB_DEV
    pair_scores = jax.random.randint(jax.random.fold_in(key, 1), (devices, devices, KB_DEV), 0, 65536) * KB_DEV + jnp.arange(KB_DEV, dtype=jnp.int32)
    ranks = jnp.sum((pair_scores[..., None, :] > pair_scores[..., :, None]).astype(jnp.int32), axis=-1)
    allowed_pair = ranks < CAP
    query_dev = owners[:, None]
    key_dev = owners[None, :]
    own_earlier = (key_dev == query_dev) & (blocks[None, :] < blocks[:, None])
    allowed_here = allowed_pair[query_dev, key_dev, within[None, :]]
    foreign = (key_dev < query_dev) & allowed_here
    candidate = own_earlier | foreign
    popular = (jax.random.randint(jax.random.fold_in(key, 2), (NBLK,), 0, 6) == 0).astype(jnp.int32)
    base = jax.random.randint(jax.random.fold_in(key, 3), (NBLK, NBLK), 0, 1024) + 4096 * popular[None, :]
    forced = foreign & (within[:, None] == 0) & ((key_dev == query_dev - 1) | (key_dev == query_dev - devices // 2))
    base = base + 65536 * forced.astype(jnp.int32)
    final = jnp.where(candidate, base * NBLK + blocks[None, :], -1)
    top_values, top_index = lax.top_k(final, NSEL - 1)
    picks = jnp.where(top_values >= 0, top_index, -1)
    return jnp.concatenate([blocks[:, None], picks], axis=1).astype(jnp.int32)


def draw_chosen(key, part):
    seq_keys = jax.vmap(lambda index: jax.random.fold_in(key, index))(jnp.arange(SEQS, dtype=jnp.int32))
    return jax.vmap(one_sequence)(seq_keys)


def block_scale(stream_key, shape, pieces, least, top_value):
    def one(position, blocks):
        draws = jax.random.uniform(jax.random.fold_in(jax.random.fold_in(stream_key, 6), position), (blocks,), jnp.float32, least / len(pieces), top_value / len(pieces))
        return jnp.repeat(jnp.exp(draws), shape[position] // blocks).reshape((-1,) + (1,) * (len(shape) - position - 1))

    loudness = one(*pieces[0])
    for cut in pieces[1:]:
        loudness = loudness * one(*cut)
    return loudness


def scatter_about(stream_key, extent, scale, limit, cuts=(), kind=jnp.bfloat16):
    drawn = scale * jax.random.normal(stream_key, extent, jnp.float32)
    if cuts:
        drawn = drawn * block_scale(stream_key, extent, cuts, -0.22, 0.18)
    return jnp.clip(drawn, -limit, limit).astype(kind)


def setup_inputs(seed: int = 0) -> dict:
    splits = jax.random.split(jax.random.key(seed), 7)
    return {
        "tokens": scatter_about(splits[0], (SEQS, LENGTH, D), 1.0, 6.0, ((0, 4), (1, 32))),
        "w_query": draw_w_query(jax.random.fold_in(splits[6], 71), 0),
        "w_key": draw_w_key(jax.random.fold_in(splits[6], 71), 0),
        "w_value": scatter_about(splits[3], (D, HEADS * HEAD_DIM), D ** -0.5, 0.125, ((1, 2),)),
        "w_out": scatter_about(splits[4], (HEADS * HEAD_DIM, D), (HEADS * HEAD_DIM) ** -0.5, 0.1875, ((0, 2),)),
        "chosen": draw_chosen(jax.random.fold_in(splits[6], 71), 0),
    }


def attend_sequence(inputs, w_query, w_key, w_value, w_out, listed):
    queries = jnp.dot(inputs, w_query, preferred_element_type=jnp.float32).astype(jnp.bfloat16)
    keys_all = jnp.dot(inputs, w_key, preferred_element_type=jnp.float32).astype(jnp.bfloat16)
    values_all = jnp.dot(inputs, w_value, preferred_element_type=jnp.float32).astype(jnp.bfloat16)
    width = queries.shape[1]
    query_blocks = queries.reshape(NBLK, BLOCK, HEADS, HEAD_DIM)
    key_blocks = keys_all.reshape(NBLK, BLOCK, HEADS, HEAD_DIM)
    value_blocks = values_all.reshape(NBLK, BLOCK, HEADS, HEAD_DIM)
    offsets = jnp.arange(BLOCK, dtype=jnp.int32)

    def one_block(args):
        query_block, row, index = args
        valid = row >= 0
        safe = jnp.where(valid, row, 0).astype(jnp.int32)
        keys_sel = key_blocks[safe].astype(jnp.float32)
        values_sel = value_blocks[safe].astype(jnp.float32)
        scores = jnp.einsum('qhd,skhd->hqsk', query_block.astype(jnp.float32), keys_sel) * (HEAD_DIM ** -0.5)
        key_pos = row[:, None] * BLOCK + offsets[None, :]
        query_pos = index * BLOCK + offsets
        allowed = valid[None, :, None] & (key_pos[None, :, :] <= query_pos[:, None, None])
        scores = jnp.where(allowed[None], scores, -jnp.inf)
        row_max = jnp.max(scores, axis=(2, 3), keepdims=True)
        exp_terms = jnp.exp(scores - row_max)
        row_sum = jnp.sum(exp_terms, axis=(2, 3), keepdims=True)
        weights = (exp_terms / row_sum).astype(jnp.bfloat16)
        attended = jnp.einsum('hqsk,skhd->qhd', weights.astype(jnp.float32), values_sel).astype(jnp.bfloat16)
        return attended.reshape(BLOCK, width), (row_max + jnp.log(row_sum))[:, :, 0, 0]

    attended, log_sums = lax.map(one_block, (query_blocks, listed, jnp.arange(NBLK, dtype=jnp.int32)))
    attended = attended.reshape(LENGTH, width)
    log_sums = jnp.transpose(log_sums, (1, 0, 2)).reshape(HEADS, LENGTH)
    share = width // N_TP
    total = jnp.zeros((LENGTH, w_out.shape[1]), jnp.float32)
    for shard in range(N_TP):
        partial_value = jnp.dot(attended[:, shard * share:(shard + 1) * share], w_out[shard * share:(shard + 1) * share],
                          preferred_element_type=jnp.float32).astype(jnp.bfloat16)
        total = total + partial_value.astype(jnp.float32)
    return total.astype(jnp.bfloat16), log_sums


def reference(tokens, w_query, w_key, w_value, w_out, chosen):
    mixed_list = []
    sums_list = []
    for seq_index in range(SEQS):
        mixed_one, sums_one = attend_sequence(tokens[seq_index], w_query, w_key, w_value, w_out, chosen[seq_index])
        mixed_list.append(mixed_one)
        sums_list.append(sums_one)
    return jnp.stack(mixed_list), jnp.stack(sums_list)
```

```python
import functools

import jax
import jax.numpy as jnp
from jax import lax
from jax.experimental import pallas as pl
from jax.experimental.pallas import tpu as pltpu
from jax.sharding import PartitionSpec as P

HEAD_DIM = 64
BLOCK = 64
NZ = 8
NY = 4
PICKS = 16
LOG2E = 1.4426950408889634
MESH = pl.DeviceIdType.MESH
BF16 = jnp.bfloat16
F32 = jnp.float32


def order(step, me_z):
    half = (step + 1) // 2
    return lax.rem(me_z + jnp.where(lax.rem(step, 2) == 1, half, NZ - half), NZ)


def kernel(
    x_hbm, wq_hbm, wk_hbm, wv_hbm, wo_hbm, chosen_ref, out_ref, logs_ref,
    x, wkv, wq, wo, kvs, land, qs, qland, cs, cland, picks, gathered, os, oland, stat, ls, lland, att,
    in_sem, wo_sem, wo_send, wo_recv, own_sem, own_out_sem, pick_sem,
    kv_send, kv_recv, q_send, q_recv, c_send, c_recv,
    y_send, y_recv, f_send, f_recv, o_send, o_recv, l_send, l_recv,
):
    kv = lax.axis_index("kv")
    core = lax.axis_index("tp")
    me_z, me_y = kv // NY, lax.rem(kv, NY)
    rows = x.shape[0]
    half = rows // 2
    blocks = rows // BLOCK
    up = me_z * NY + lax.rem(me_y + 1, NY)
    down = me_z * NY + lax.rem(me_y + NY - 1, NY)
    below = lax.rem(me_y + NY - 1, NY)
    above = lax.rem(me_y + 1, NY)

    def at(z):
        return z * NY + me_y

    x_copy = pltpu.make_async_copy(x_hbm, x, in_sem.at[0])
    x_copy.start()
    w_copies = []
    for p in range(4):
        pair = []
        for i, src in enumerate((wk_hbm, wv_hbm)):
            c = pltpu.make_async_copy(
                src.at[:, pl.ds(p * 128, 128)], wkv.at[p, :, pl.ds(i * 128, 128)], in_sem.at[1 + 2 * p + i]
            )
            c.start()
            pair.append(c)
        w_copies.append(pair)
    wq_copy = pltpu.make_async_copy(wq_hbm, wq, in_sem.at[9])
    wq_copy.start()

    barrier = pltpu.get_barrier_semaphore()
    for k in range(NZ):
        z = lax.rem(me_z + k, NZ)
        for c in range(2):
            if k == 0 and c == 0:
                pl.semaphore_signal(barrier, inc=1, device_id={"tp": 1 - core}, device_id_type=MESH)
            elif k > 0:
                pl.semaphore_signal(barrier, inc=1, device_id={"kv": at(z), "tp": c}, device_id_type=MESH)
    for peer in (up, down):
        pl.semaphore_signal(barrier, inc=1, device_id={"kv": peer}, device_id_type=MESH)

    cs[...] = jnp.zeros_like(cs)
    cs[:, 0:PICKS] = jnp.maximum(chosen_ref[...], 0)
    lane = lax.broadcasted_iota(jnp.int32, (rows, 128), 1)
    low = lane < HEAD_DIM

    x_copy.wait()
    for p in range(4):
        for c in w_copies[p]:
            c.wait()

    def project_pair(p, carry):
        both = jnp.dot(x[...], wkv[p], preferred_element_type=F32)
        kp, vp = both[:, 0:128], both[:, 128:256]
        kvs[2 * p] = jnp.where(low, kp, pltpu.roll(vp, HEAD_DIM, 1)).astype(BF16).reshape(blocks, BLOCK, 128)
        kvs[2 * p + 1] = jnp.where(low, pltpu.roll(kp, HEAD_DIM, 1), vp).astype(BF16).reshape(blocks, BLOCK, 128)
        return carry

    lax.fori_loop(0, 4, project_pair, 0)
    pl.semaphore_wait(barrier, 2 * NZ + 1)

    def kv_copy(z):
        return pltpu.make_async_remote_copy(
            src_ref=kvs.at[z], dst_ref=land.at[pl.ds(kv * blocks, blocks)], send_sem=kv_send.at[z],
            recv_sem=kv_recv.at[me_z], device_id={"kv": at(z)}, device_id_type=MESH,
        )

    def kv_arrival(z):
        return pltpu.make_async_remote_copy(
            src_ref=kvs.at[z], dst_ref=land.at[pl.ds(at(z) * blocks, blocks)], send_sem=kv_send.at[z],
            recv_sem=kv_recv.at[z], device_id={"kv": at(z)}, device_id_type=MESH,
        )

    def q_copy(z, src):
        return pltpu.make_async_remote_copy(
            src_ref=qs.at[z], dst_ref=qland.at[src], send_sem=q_send.at[z],
            recv_sem=q_recv.at[src], device_id={"kv": at(z)}, device_id_type=MESH,
        )

    def c_copy(z, src):
        return pltpu.make_async_remote_copy(
            src_ref=cs, dst_ref=cland.at[src], send_sem=c_send.at[z],
            recv_sem=c_recv.at[src], device_id={"kv": at(z)}, device_id_type=MESH,
        )

    own_kv = pltpu.make_async_copy(kvs.at[me_z], land.at[pl.ds(kv * blocks, blocks)], own_sem.at[0])
    own_kv.start()
    own_c = pltpu.make_async_copy(cs, cland.at[me_z], own_sem.at[1])
    own_c.start()
    for t in range(1, NZ):
        c_copy(order(t, me_z), me_z).start()
    for t in range(1, NZ):
        kv_copy(order(t, me_z)).start()

    wo_rows = wo_hbm.shape[0]
    wo_mine = wo.at[pl.ds(core * wo_rows, wo_rows)]
    wo_local = pltpu.make_async_copy(wo_hbm, wo_mine, wo_sem)
    wo_local.start()
    wo_remote = pltpu.make_async_remote_copy(
        src_ref=wo_hbm, dst_ref=wo_mine, send_sem=wo_send, recv_sem=wo_recv,
        device_id={"tp": 1 - core}, device_id_type=MESH,
    )
    wo_remote.start()

    wq_copy.wait()

    def project_queries(i, carry):
        res = jnp.dot(x[...], wq[:, pl.ds(pl.multiple_of(i * 256, 256), 256)], preferred_element_type=F32)
        lo = low[:half]
        for u in range(2):
            top, bot = res[:half, u * 128:(u + 1) * 128], res[half:, u * 128:(u + 1) * 128]
            qs[4 * i + 2 * u] = jnp.where(lo, top, pltpu.roll(bot, HEAD_DIM, 1)).astype(BF16)
            qs[4 * i + 2 * u + 1] = jnp.where(lo, pltpu.roll(top, HEAD_DIM, 1), bot).astype(BF16)
        return carry

    lax.fori_loop(0, 2, project_queries, 0)
    own_q = pltpu.make_async_copy(qs.at[me_z], qland.at[me_z], own_sem.at[2])
    own_q.start()
    for t in range(1, NZ):
        q_copy(order(t, me_z), me_z).start()

    def y_copy(z, way):
        rng = pl.ds(at(z) * blocks, blocks)
        return pltpu.make_async_remote_copy(
            src_ref=land.at[rng], dst_ref=land.at[rng], send_sem=y_send.at[z, way],
            recv_sem=y_recv.at[z, way], device_id={"kv": (up, down)[way]}, device_id_type=MESH,
        )

    def y_arrival(z, way):
        rng = pl.ds((z * NY + (below, above)[way]) * blocks, blocks)
        return pltpu.make_async_remote_copy(
            src_ref=land.at[rng], dst_ref=land.at[rng], send_sem=y_send.at[z, way],
            recv_sem=y_recv.at[z, way], device_id={"kv": (up, down)[way]}, device_id_type=MESH,
        )

    def f_copy(z, way):
        rng = pl.ds((z * NY + (below, above)[way]) * blocks + way * (blocks // 2), blocks // 2)
        return pltpu.make_async_remote_copy(
            src_ref=land.at[rng], dst_ref=land.at[rng], send_sem=f_send.at[z, way],
            recv_sem=f_recv.at[z, way], device_id={"kv": (up, down)[way]}, device_id_type=MESH,
        )

    far = lax.rem(me_y + 2, NY)

    def f_arrival(z, way):
        rng = pl.ds((z * NY + far) * blocks + way * (blocks // 2), blocks // 2)
        return pltpu.make_async_remote_copy(
            src_ref=land.at[rng], dst_ref=land.at[rng], send_sem=f_send.at[z, way],
            recv_sem=f_recv.at[z, way], device_id={"kv": (up, down)[way]}, device_id_type=MESH,
        )

    own_kv.wait()
    for t in range(NZ + 1):
        if t < NZ:
            z = order(t, me_z)
            if t > 0:
                kv_arrival(z).wait_recv()
            for way in range(2):
                y_copy(z, way).start()
        if t > 0:
            z = order(t - 1, me_z)
            for way in range(2):
                y_arrival(z, way).wait_recv()
                f_copy(z, way).start()
    for z in range(NZ):
        for way in range(2):
            f_arrival(z, way).wait_recv()

    own_c.wait()
    own_q.wait()
    for t in range(1, NZ):
        z = order(t, me_z)
        c_copy(z, z).wait_recv()
    to_scalars = pltpu.make_async_copy(cland, picks, pick_sem)
    to_scalars.start()
    to_scalars.wait()

    row_iota = lax.broadcasted_iota(jnp.int32, (128, 128), 0)
    lane_iota = lax.broadcasted_iota(jnp.int32, (128, 128), 1)
    low64 = lax.broadcasted_iota(jnp.int32, (BLOCK, 128), 1) < HEAD_DIM
    key_iota = lax.broadcasted_iota(jnp.int32, (128, PICKS * BLOCK), 1)
    row_col = lax.broadcasted_iota(jnp.int32, (128, 1), 0)
    hidden = (lane_iota < BLOCK) & (lane_iota > lax.rem(row_iota, BLOCK))
    zero = jnp.zeros((BLOCK, 128), BF16)

    def o_copy(g, to):
        return pltpu.make_async_remote_copy(
            src_ref=os.at[g, to], dst_ref=oland.at[core * NZ + me_z], send_sem=o_send.at[g, to],
            recv_sem=o_recv.at[core * NZ + me_z], device_id={"kv": at(g), "tp": to}, device_id_type=MESH,
        )

    def l_copy(g, src):
        return pltpu.make_async_remote_copy(
            src_ref=ls.at[g], dst_ref=lland.at[src], send_sem=l_send.at[g],
            recv_sem=l_recv.at[src], device_id={"kv": at(g)}, device_id_type=MESH,
        )

    def attend_group(t, carry):
        g = order(t, me_z)

        @pl.when(t > 0)
        def _():
            q_copy(g, g).wait_recv()

        def attend_pair(j, carry):
            for s in range(PICKS):
                for i in range(2):
                    gathered[pl.ds(s * BLOCK, BLOCK), pl.ds(i * 128, 128)] = land[picks[g, j + 4 * i, s]]
            tile = qland[g, pl.ds(pl.multiple_of(j * BLOCK, BLOCK), BLOCK), :].astype(F32)
            first = jnp.where(low64, tile, 0.0).astype(BF16)
            second = jnp.where(low64, pltpu.roll(tile, HEAD_DIM, 1), 0.0).astype(BF16)
            lhs = jnp.concatenate(
                [jnp.concatenate([first, zero], axis=1), jnp.concatenate([zero, second], axis=1)], axis=0
            )
            s = lax.dot_general(lhs, gathered[...], (((1,), (1,)), ((), ())), preferred_element_type=F32)
            device = g * NY + me_y
            limit = (jnp.where(row_col < BLOCK, j, j + 4) + 2 * device + 1) * BLOCK
            s = jnp.where(key_iota < limit, s, -jnp.inf)
            s = jnp.concatenate([jnp.where(hidden, -jnp.inf, s[:, 0:128]), s[:, 128:]], axis=1)
            peak = jnp.max(s, axis=1, keepdims=True)
            e = jnp.exp2((s - peak) * (LOG2E * HEAD_DIM ** -0.5))
            total = jnp.sum(e, axis=1, keepdims=True)
            o = jnp.dot(e.astype(BF16), gathered[...], preferred_element_type=F32) * (1.0 / total)
            log_sum = peak * HEAD_DIM ** -0.5 + jnp.log(total)
            stat[...] = jnp.where(lane_iota == j, log_sum, stat[...])
            place = pl.ds(pl.multiple_of(lax.rem(j, 2) * BLOCK, BLOCK), BLOCK)
            for i in range(2):
                part = o[i * BLOCK:(i + 1) * BLOCK, i * 128:(i + 1) * 128]
                old = os[g, i, place, :].astype(F32)
                left = jnp.where(j < 2, pltpu.roll(part, HEAD_DIM, 1), old)
                os[g, i, place, :] = jnp.where(low64, left, part).astype(BF16)
            return carry

        lax.fori_loop(0, 4, attend_pair, 0)
        ls[g] = stat[...].T[0:8]

        @pl.when(g != me_z)
        def _():
            o_copy(g, 0).start()
            o_copy(g, 1).start()
            l_copy(g, me_z).start()

        @pl.when(g == me_z)
        def _():
            o_copy(g, 1 - core).start()
            pltpu.make_async_copy(os.at[g, core], oland.at[core * NZ + me_z], own_out_sem.at[0]).start()
            pltpu.make_async_copy(ls.at[g], lland.at[me_z], own_out_sem.at[1]).start()

        return carry

    stat[...] = jnp.zeros_like(stat)
    os[...] = jnp.zeros_like(os)
    lax.fori_loop(0, NZ, attend_group, 0)

    def o_arrival(head):
        return pltpu.make_async_remote_copy(
            src_ref=os.at[0, 0], dst_ref=oland.at[head], send_sem=o_send.at[0, 0],
            recv_sem=o_recv.at[head], device_id={"tp": 1 - core}, device_id_type=MESH,
        )

    pltpu.make_async_copy(os.at[me_z, core], oland.at[core * NZ + me_z], own_out_sem.at[0]).wait()
    pltpu.make_async_copy(ls.at[me_z], lland.at[me_z], own_out_sem.at[1]).wait()
    for t in range(1, NZ):
        z = order(t, me_z)
        o_arrival(core * NZ + z).wait_recv()
        l_copy(z, z).wait_recv()
    for z in range(NZ):
        o_arrival((1 - core) * NZ + z).wait_recv()
    low128 = lane_iota < HEAD_DIM
    for i in range(NZ):
        a, b = oland[2 * i].astype(F32), oland[2 * i + 1].astype(F32)
        cols = pl.ds(i * 128, 128)
        att[0:128, cols] = jnp.where(low128, a, pltpu.roll(b, HEAD_DIM, 1)).astype(BF16)
        att[128:256, cols] = jnp.where(low128, pltpu.roll(a, HEAD_DIM, 1), b).astype(BF16)
    low8 = low128[:8]
    for h in range(NZ):
        mine = lland[h]
        turned = pltpu.roll(mine, HEAD_DIM, 1)
        for q, (left, right) in enumerate(
            ((mine[0:1], turned[1:2]), (mine[2:3], turned[3:4]), (turned[0:1], mine[1:2]), (turned[2:3], mine[3:4]))
        ):
            logs_ref[h:h + 1, q * 128:(q + 1) * 128] = jnp.where(low8[:1], left, right)
    wo_local.wait()
    wo_remote.wait_send()
    pltpu.make_async_remote_copy(
        src_ref=wo_hbm, dst_ref=wo.at[pl.ds((1 - core) * wo_rows, wo_rows)], send_sem=wo_send, recv_sem=wo_recv,
        device_id={"tp": 1 - core}, device_id_type=MESH,
    ).wait_recv()

    def project_out(n, carry):
        cols = pl.ds(pl.multiple_of(n * 512, 512), 512)
        out_ref[:, cols] = jnp.dot(att[...], wo[:, cols], preferred_element_type=F32).astype(BF16)
        return carry

    lax.fori_loop(0, out_ref.shape[1] // 512, project_out, 0)

    for t in range(1, NZ):
        z = order(t, me_z)
        kv_copy(z).wait_send()
        q_copy(z, me_z).wait_send()
        c_copy(z, me_z).wait_send()
        o_copy(z, 0).wait_send()
        o_copy(z, 1).wait_send()
        l_copy(z, me_z).wait_send()
    o_copy(me_z, 1 - core).wait_send()
    for z in range(NZ):
        for way in range(2):
            y_copy(z, way).wait_send()
            f_copy(z, way).wait_send()


def on_device(tokens, w_query, w_key, w_value, w_out, chosen):
    rows, model = tokens.shape[1:]
    width = w_query.shape[1]
    hbm = pl.BlockSpec(memory_space=pl.ANY)
    vmem = pl.BlockSpec(memory_space=pltpu.VMEM)
    dma = pltpu.SemaphoreType.DMA
    mixed, log_sums = pl.pallas_call(
        kernel,
        out_shape=(
            jax.ShapeDtypeStruct((rows // 2, model), BF16),
            jax.ShapeDtypeStruct((width // HEAD_DIM, rows), F32),
        ),
        in_specs=[hbm] * 5 + [vmem],
        out_specs=(vmem, vmem),
        scratch_shapes=[
            pltpu.VMEM((rows, model), BF16),
            pltpu.VMEM((4, model, 256), BF16),
            pltpu.VMEM((model, width), BF16),
            pltpu.VMEM((2 * width, model), BF16),
            pltpu.VMEM((NZ, rows // BLOCK, BLOCK, 128), BF16),
            pltpu.VMEM((NZ * NY * rows // BLOCK, BLOCK, 128), BF16),
            pltpu.VMEM((NZ, rows // 2, 128), BF16),
            pltpu.VMEM((NZ, rows // 2, 128), BF16),
            pltpu.VMEM((8, 128), jnp.int32),
            pltpu.VMEM((NZ, 8, 128), jnp.int32),
            pltpu.SMEM((NZ, 8, 128), jnp.int32),
            pltpu.VMEM((PICKS * BLOCK, 256), BF16),
            pltpu.VMEM((NZ, 2, 128, 128), BF16),
            pltpu.VMEM((2 * NZ, 128, 128), BF16),
            pltpu.VMEM((128, 128), F32),
            pltpu.VMEM((NZ, 8, 128), F32),
            pltpu.VMEM((NZ, 8, 128), F32),
            pltpu.VMEM((rows // 2, 2 * width), BF16),
            dma((10,)), dma, dma, dma, dma((3,)), dma((2,)), dma,
            dma((NZ,)), dma((NZ,)), dma((NZ,)), dma((NZ,)), dma((NZ,)), dma((NZ,)),
            dma((NZ, 2)), dma((NZ, 2)), dma((NZ, 2)), dma((NZ, 2)),
            dma((NZ, 2)), dma((2 * NZ,)), dma((NZ,)), dma((NZ,)),
        ],
        compiler_params=pltpu.CompilerParams(collective_id=0, has_side_effects=True, vmem_limit_bytes=48 * 2**20),
        name="heads_over_z",
    )(tokens[0], w_query, w_key, w_value, w_out, chosen[0])
    return mixed[None], log_sums[None]


def solution(mesh):
    return jax.shard_map(
        on_device,
        mesh=mesh,
        in_specs=(
            P("dp", "kv", None),
            P(None, "tp"),
            P(None, "tp"),
            P(None, "tp"),
            P("tp", None),
            P("dp", "kv", None),
        ),
        out_specs=(P("dp", ("kv", "tp"), None), P("dp", "tp", "kv")),
        check_vma=False,
    )
```

```python
import functools

import jax
import jax.numpy as jnp
from jax import lax
from jax.experimental import pallas as pl
from jax.experimental.pallas import tpu as pltpu
from jax.sharding import PartitionSpec as P

HEAD_DIM = 64
BLOCK = 64
NZ = 8
NY = 4
PICKS = 16
LOG2E = 1.4426950408889634
MESH = pl.DeviceIdType.MESH
BF16 = jnp.bfloat16
F32 = jnp.float32


def arrival_order(step, me_z):
    turn = step // 2
    second = step - 2 * turn
    parity = lax.rem(me_z, 2)
    pair = lax.rem(me_z // 2 + jnp.where(turn == 1, 3, jnp.where(turn == 2, 1, jnp.where(turn == 3, 2, 0))), NZ // 2)
    swapped = lax.rem(parity + 1 - second + NZ, 2)
    straight = lax.rem(parity + second, 2)
    member = jnp.where(turn == 0, straight, jnp.where(turn == 1, 1 - second, jnp.where(turn == 2, second, swapped)))
    return pair * 2 + member


def kernel(
    x_hbm, wq_hbm, wk_hbm, wv_hbm, wo_hbm, chosen_ref, out_ref, logs_ref,
    x, wkv, wq, wo, kvs, land, qs, qland, cs, cland, picks, relay_kv, relay_q, scores, os, oland, stat, ls, lland, att,
    in_sem, wo_sem, wo_send, wo_recv, own_sem, own_out_sem, pick_sem,
    kv_send, kv_recv, q_send, q_recv, c_send, c_recv,
    relay_send, relay_recv, y_send, y_recv, f_send, f_recv, o_send, o_recv, l_send, l_recv,
):
    kv = lax.axis_index("kv")
    core = lax.axis_index("tp")
    me_z, me_y = kv // NY, lax.rem(kv, NY)
    rows = x.shape[0]
    half = rows // 2
    blocks = rows // BLOCK
    up = me_z * NY + lax.rem(me_y + 1, NY)
    down = me_z * NY + lax.rem(me_y + NY - 1, NY)
    below = lax.rem(me_y + NY - 1, NY)
    above = lax.rem(me_y + 1, NY)

    def at(z):
        return z * NY + me_y

    x_copy = pltpu.make_async_copy(x_hbm, x, in_sem.at[0])
    x_copy.start()
    w_copies = []
    for n, turn in enumerate((0, 1, 3, 2)):
        pair = lax.rem(me_z // 2 + turn, NZ // 2)
        cols = pl.ds(pl.multiple_of(pair * 128, 128), 128)
        copies = []
        for i, src in enumerate((wk_hbm, wv_hbm)):
            copies.append(
                pltpu.make_async_copy(src.at[:, cols], wkv.at[n, :, pl.ds(i * 128, 128)], in_sem.at[1 + 2 * n + i])
            )
            copies[-1].start()
        w_copies.append((pair, copies))
    wq_copy = pltpu.make_async_copy(wq_hbm, wq, in_sem.at[9])
    wq_copy.start()

    barrier = pltpu.get_barrier_semaphore()
    for k in range(NZ):
        z = lax.rem(me_z + k, NZ)
        for c in range(2):
            if k == 0 and c == 0:
                pl.semaphore_signal(barrier, inc=1, device_id={"tp": 1 - core}, device_id_type=MESH)
            elif k > 0:
                pl.semaphore_signal(barrier, inc=1, device_id={"kv": at(z), "tp": c}, device_id_type=MESH)
    for peer in (up, down):
        pl.semaphore_signal(barrier, inc=1, device_id={"kv": peer}, device_id_type=MESH)

    cs[...] = jnp.zeros_like(cs)
    cs[:, 0:PICKS] = jnp.maximum(chosen_ref[...], 0)
    lane = lax.broadcasted_iota(jnp.int32, (rows, 128), 1)
    low = lane < HEAD_DIM

    far = lax.rem(me_z + NZ // 2, NZ)
    left = lax.rem(me_z + NZ - 1, NZ)
    right = lax.rem(me_z + 1, NZ)

    def kv_copy(z):
        return pltpu.make_async_remote_copy(
            src_ref=kvs.at[z], dst_ref=land.at[pl.ds(kv * blocks, blocks)], send_sem=kv_send.at[z],
            recv_sem=kv_recv.at[me_z], device_id={"kv": at(z)}, device_id_type=MESH,
        )

    def kv_arrival(z):
        return pltpu.make_async_remote_copy(
            src_ref=kvs.at[z], dst_ref=land.at[pl.ds(at(z) * blocks, blocks)], send_sem=kv_send.at[z],
            recv_sem=kv_recv.at[z], device_id={"kv": at(z)}, device_id_type=MESH,
        )

    def q_copy(z, src):
        return pltpu.make_async_remote_copy(
            src_ref=qs.at[z], dst_ref=qland.at[src], send_sem=q_send.at[z],
            recv_sem=q_recv.at[src], device_id={"kv": at(z)}, device_id_type=MESH,
        )

    def c_copy(z, src):
        return pltpu.make_async_remote_copy(
            src_ref=cs, dst_ref=cland.at[src], send_sem=c_send.at[z],
            recv_sem=c_recv.at[src], device_id={"kv": at(z)}, device_id_type=MESH,
        )

    def kv_first_leg():
        return pltpu.make_async_remote_copy(
            src_ref=kvs.at[far], dst_ref=relay_kv, send_sem=kv_send.at[far],
            recv_sem=relay_recv.at[0], device_id={"kv": at(left)}, device_id_type=MESH,
        )

    def kv_second_leg():
        return pltpu.make_async_remote_copy(
            src_ref=relay_kv, dst_ref=land.at[pl.ds(at(right) * blocks, blocks)], send_sem=relay_send.at[0],
            recv_sem=kv_recv.at[right], device_id={"kv": at(lax.rem(right + NZ // 2, NZ))}, device_id_type=MESH,
        )

    def q_first_leg():
        return pltpu.make_async_remote_copy(
            src_ref=qs.at[far], dst_ref=relay_q, send_sem=q_send.at[far],
            recv_sem=relay_recv.at[1], device_id={"kv": at(left)}, device_id_type=MESH,
        )

    def q_second_leg():
        return pltpu.make_async_remote_copy(
            src_ref=relay_q, dst_ref=qland.at[right], send_sem=relay_send.at[1],
            recv_sem=q_recv.at[right], device_id={"kv": at(lax.rem(right + NZ // 2, NZ))}, device_id_type=MESH,
        )

    def y_copy(z, way, src=None):
        rng = pl.ds(at(z) * blocks, blocks)
        return pltpu.make_async_remote_copy(
            src_ref=land.at[rng] if src is None else src, dst_ref=land.at[rng], send_sem=y_send.at[z, way],
            recv_sem=y_recv.at[z, way], device_id={"kv": (up, down)[way]}, device_id_type=MESH,
        )

    own_kv = pltpu.make_async_copy(kvs.at[me_z], land.at[pl.ds(kv * blocks, blocks)], own_sem.at[0])
    own_c = pltpu.make_async_copy(cs, cland.at[me_z], own_sem.at[1])
    x_copy.wait()
    parity = lax.rem(me_z, 2)
    for n, (pair, copies) in enumerate(w_copies):
        for c in copies:
            c.wait()
        both = jnp.dot(x[...], wkv[n], preferred_element_type=F32)
        kp, vp = both[:, 0:128], both[:, 128:256]
        kvs[2 * pair] = jnp.where(low, kp, pltpu.roll(vp, HEAD_DIM, 1)).astype(BF16).reshape(blocks, BLOCK, 128)
        kvs[2 * pair + 1] = jnp.where(low, pltpu.roll(kp, HEAD_DIM, 1), vp).astype(BF16).reshape(blocks, BLOCK, 128)
        if n == 0:
            pl.semaphore_wait(barrier, 2 * NZ + 1)
            own_c.start()
            for t in range(1, NZ):
                c_copy(arrival_order(t, me_z), me_z).start()
            for way in range(2):
                y_copy(me_z, way, kvs.at[me_z]).start()
            own_kv.start()
            kv_copy(2 * pair + 1 - parity).start()
        elif n < 3:
            for m in ((0, 1) if n == 1 else (1, 0)):
                kv_copy(2 * pair + m).start()
        else:
            @pl.when(core == 0)
            def _():
                kv_copy(far).start()

            @pl.when(core == 1)
            def _():
                kv_first_leg().start()

            kv_copy(2 * pair + 1 - parity).start()

    wo_rows = wo_hbm.shape[0]
    wo_mine = wo.at[pl.ds(core * wo_rows, wo_rows)]
    wo_local = pltpu.make_async_copy(wo_hbm, wo_mine, wo_sem)
    wo_local.start()
    wo_remote = pltpu.make_async_remote_copy(
        src_ref=wo_hbm, dst_ref=wo_mine, send_sem=wo_send, recv_sem=wo_recv,
        device_id={"tp": 1 - core}, device_id_type=MESH,
    )
    wo_remote.start()

    wq_copy.wait()

    def project_queries(i, carry):
        res = jnp.dot(x[...], wq[:, pl.ds(pl.multiple_of(i * 256, 256), 256)], preferred_element_type=F32)
        lo = low[:half]
        for u in range(2):
            top, bot = res[:half, u * 128:(u + 1) * 128], res[half:, u * 128:(u + 1) * 128]
            qs[4 * i + 2 * u] = jnp.where(lo, top, pltpu.roll(bot, HEAD_DIM, 1)).astype(BF16)
            qs[4 * i + 2 * u + 1] = jnp.where(lo, pltpu.roll(top, HEAD_DIM, 1), bot).astype(BF16)
        return carry

    lax.fori_loop(0, 2, project_queries, 0)
    own_q = pltpu.make_async_copy(qs.at[me_z], qland.at[me_z], own_sem.at[2])
    own_q.start()

    @pl.when(core == 0)
    def _():
        q_copy(far, me_z).start()

    @pl.when(core == 1)
    def _():
        q_first_leg().start()

    for t in range(6, 0, -1):
        q_copy(arrival_order(t, me_z), me_z).start()

    def y_arrival(z, way):
        rng = pl.ds((z * NY + (below, above)[way]) * blocks, blocks)
        return pltpu.make_async_remote_copy(
            src_ref=land.at[rng], dst_ref=land.at[rng], send_sem=y_send.at[z, way],
            recv_sem=y_recv.at[z, way], device_id={"kv": (up, down)[way]}, device_id_type=MESH,
        )

    def f_copy(z, way):
        rng = pl.ds((z * NY + (below, above)[way]) * blocks + way * (blocks // 2), blocks // 2)
        return pltpu.make_async_remote_copy(
            src_ref=land.at[rng], dst_ref=land.at[rng], send_sem=f_send.at[z, way],
            recv_sem=f_recv.at[z, way], device_id={"kv": (up, down)[way]}, device_id_type=MESH,
        )

    across = lax.rem(me_y + 2, NY)

    def f_arrival(z, way):
        rng = pl.ds((z * NY + across) * blocks + way * (blocks // 2), blocks // 2)
        return pltpu.make_async_remote_copy(
            src_ref=land.at[rng], dst_ref=land.at[rng], send_sem=f_send.at[z, way],
            recv_sem=f_recv.at[z, way], device_id={"kv": (up, down)[way]}, device_id_type=MESH,
        )

    own_kv.wait()
    for t in range(1, NZ + 1):
        if t < NZ:
            z = arrival_order(t, me_z)
            kv_arrival(z).wait_recv()
            for way in range(2):
                y_copy(z, way).start()
        z = arrival_order(t - 1, me_z)
        for way in range(2):
            y_arrival(z, way).wait_recv()
            f_copy(z, way).start()
        if t == 5:
            @pl.when(core == 1)
            def _():
                kv_first_leg().wait_recv()
                kv_second_leg().start()
        if t == 6:
            @pl.when(core == 1)
            def _():
                q_first_leg().wait_recv()
                q_second_leg().start()
    for z in range(NZ):
        for way in range(2):
            f_arrival(z, way).wait_recv()

    own_c.wait()
    own_q.wait()
    for t in range(1, NZ):
        z = arrival_order(t, me_z)
        c_copy(z, z).wait_recv()
    to_scalars = pltpu.make_async_copy(cland, picks, pick_sem)
    to_scalars.start()
    to_scalars.wait()

    lane_iota = lax.broadcasted_iota(jnp.int32, (128, 128), 1)
    low64 = lax.broadcasted_iota(jnp.int32, (BLOCK, 128), 1) < HEAD_DIM
    zero = jnp.zeros((BLOCK, 128), BF16)

    def o_copy(g, to):
        return pltpu.make_async_remote_copy(
            src_ref=os.at[g, to], dst_ref=oland.at[core * NZ + me_z], send_sem=o_send.at[g, to],
            recv_sem=o_recv.at[core * NZ + me_z], device_id={"kv": at(g), "tp": to}, device_id_type=MESH,
        )

    def l_copy(g, src):
        return pltpu.make_async_remote_copy(
            src_ref=ls.at[g], dst_ref=lland.at[src], send_sem=l_send.at[g],
            recv_sem=l_recv.at[src], device_id={"kv": at(g)}, device_id_type=MESH,
        )

    key_row = lax.broadcasted_iota(jnp.int32, (1, PICKS * BLOCK), 1)
    diagonal = jnp.where(
        lax.broadcasted_iota(jnp.int32, (BLOCK, 128), 1) >= BLOCK, 0.0,
        jnp.where(
            lax.broadcasted_iota(jnp.int32, (BLOCK, 128), 1) > lax.broadcasted_iota(jnp.int32, (BLOCK, 128), 0),
            -jnp.inf, 0.0,
        ),
    )

    def listed(g, j):
        return jnp.concatenate([land[picks[g, j, s]] for s in range(PICKS)], axis=0)

    def score(g, j, slot):
        tile = qland[g, j * BLOCK:(j + 1) * BLOCK, :].astype(F32)
        halves = (tile, pltpu.roll(tile, HEAD_DIM, 1))
        first, second = [jnp.where(low64, h, 0.0).astype(BF16) for h in halves]
        lhs = jnp.concatenate([jnp.concatenate([first, zero], axis=1), jnp.concatenate([zero, second], axis=1)], axis=0)
        keys = jnp.concatenate([listed(g, j), listed(g, j + 4)], axis=1)
        res = lax.dot_general(lhs, keys, (((1,), (1,)), ((), ())), preferred_element_type=F32)
        scores[slot, 0] = res[:BLOCK]
        scores[slot, 1] = res[BLOCK:]

    def finish(g, j, slot):
        device = g * NY + me_y
        for i in range(2):
            bias = jnp.where(key_row < (j + 4 * i + 2 * device + 1) * BLOCK, 0.0, -jnp.inf)
            s = scores[slot, i] + bias
            s = jnp.concatenate([s[:, 0:128] + diagonal, s[:, 128:]], axis=1)
            peak = jnp.max(s, axis=1, keepdims=True)
            e = jnp.exp2((s - peak) * (LOG2E * HEAD_DIM ** -0.5))
            total = jnp.sum(e, axis=1, keepdims=True)
            part = jnp.dot(e.astype(BF16), listed(g, j + 4 * i), preferred_element_type=F32) * (1.0 / total)
            log_sum = peak * HEAD_DIM ** -0.5 + jnp.log(total)
            band = slice(i * BLOCK, (i + 1) * BLOCK)
            stat[band, :] = jnp.where(lane_iota[band] == j, log_sum, stat[band, :])
            place = slice((j % 2) * BLOCK, (j % 2 + 1) * BLOCK)
            if j < 2:
                os[g, i, place, :] = pltpu.roll(part, HEAD_DIM, 1).astype(BF16)
            else:
                os[g, i, place, :] = jnp.where(low64, os[g, i, place, :].astype(F32), part).astype(BF16)

    def attend_group(t, carry):
        g = arrival_order(NZ - 1 - t, me_z)
        following = arrival_order(jnp.maximum(NZ - 2 - t, 0), me_z)

        @pl.when(t < NZ - 2)
        def _():
            q_copy(following, following).wait_recv()

        for j in range(4):
            if j < 3:
                score(g, j + 1, (j + 1) % 2)
            else:
                score(following, 0, 0)
            finish(g, j, j % 2)
        ls[g] = stat[...].T[0:8]

        @pl.when(g != me_z)
        def _():
            o_copy(g, 0).start()
            o_copy(g, 1).start()
            l_copy(g, me_z).start()

        @pl.when(g == me_z)
        def _():
            o_copy(g, 1 - core).start()
            pltpu.make_async_copy(os.at[g, core], oland.at[core * NZ + me_z], own_out_sem.at[0]).start()
            pltpu.make_async_copy(ls.at[g], lland.at[me_z], own_out_sem.at[1]).start()

        return carry

    stat[...] = jnp.zeros_like(stat)
    os[...] = jnp.zeros_like(os)
    q_copy(far, far).wait_recv()
    score(far, 0, 0)
    lax.fori_loop(0, NZ, attend_group, 0)

    def o_arrival(head):
        return pltpu.make_async_remote_copy(
            src_ref=os.at[0, 0], dst_ref=oland.at[head], send_sem=o_send.at[0, 0],
            recv_sem=o_recv.at[head], device_id={"tp": 1 - core}, device_id_type=MESH,
        )

    pltpu.make_async_copy(os.at[me_z, core], oland.at[core * NZ + me_z], own_out_sem.at[0]).wait()
    pltpu.make_async_copy(ls.at[me_z], lland.at[me_z], own_out_sem.at[1]).wait()
    for t in range(1, NZ):
        z = arrival_order(t, me_z)
        o_arrival(core * NZ + z).wait_recv()
        l_copy(z, z).wait_recv()
    for z in range(NZ):
        o_arrival((1 - core) * NZ + z).wait_recv()
    low128 = lane_iota < HEAD_DIM
    for i in range(NZ):
        a, b = oland[2 * i].astype(F32), oland[2 * i + 1].astype(F32)
        cols = pl.ds(i * 128, 128)
        att[0:128, cols] = jnp.where(low128, a, pltpu.roll(b, HEAD_DIM, 1)).astype(BF16)
        att[128:256, cols] = jnp.where(low128, pltpu.roll(a, HEAD_DIM, 1), b).astype(BF16)
    low8 = low128[:8]
    for h in range(NZ):
        mine = lland[h]
        turned = pltpu.roll(mine, HEAD_DIM, 1)
        for q, (one, other) in enumerate(
            ((mine[0:1], turned[1:2]), (mine[2:3], turned[3:4]), (turned[0:1], mine[1:2]), (turned[2:3], mine[3:4]))
        ):
            logs_ref[h:h + 1, q * 128:(q + 1) * 128] = jnp.where(low8[:1], one, other)
    wo_local.wait()
    wo_remote.wait_send()
    pltpu.make_async_remote_copy(
        src_ref=wo_hbm, dst_ref=wo.at[pl.ds((1 - core) * wo_rows, wo_rows)], send_sem=wo_send, recv_sem=wo_recv,
        device_id={"tp": 1 - core}, device_id_type=MESH,
    ).wait_recv()

    def project_out(n, carry):
        cols = pl.ds(pl.multiple_of(n * 512, 512), 512)
        out_ref[:, cols] = jnp.dot(att[...], wo[:, cols], preferred_element_type=F32).astype(BF16)
        return carry

    lax.fori_loop(0, out_ref.shape[1] // 512, project_out, 0)

    for t in range(1, NZ):
        z = arrival_order(t, me_z)
        kv_copy(z).wait_send()
        q_copy(z, me_z).wait_send()
        c_copy(z, me_z).wait_send()
        o_copy(z, 0).wait_send()
        o_copy(z, 1).wait_send()
        l_copy(z, me_z).wait_send()
    o_copy(me_z, 1 - core).wait_send()

    @pl.when(core == 1)
    def _():
        kv_second_leg().wait_send()
        q_second_leg().wait_send()

    for z in range(NZ):
        for way in range(2):
            y_copy(z, way).wait_send()
            f_copy(z, way).wait_send()


def on_device(tokens, w_query, w_key, w_value, w_out, chosen):
    rows, model = tokens.shape[1:]
    width = w_query.shape[1]
    hbm = pl.BlockSpec(memory_space=pl.ANY)
    vmem = pl.BlockSpec(memory_space=pltpu.VMEM)
    dma = pltpu.SemaphoreType.DMA
    mixed, log_sums = pl.pallas_call(
        kernel,
        out_shape=(
            jax.ShapeDtypeStruct((rows // 2, model), BF16),
            jax.ShapeDtypeStruct((width // HEAD_DIM, rows), F32),
        ),
        in_specs=[hbm] * 5 + [vmem],
        out_specs=(vmem, vmem),
        scratch_shapes=[
            pltpu.VMEM((rows, model), BF16),
            pltpu.VMEM((4, model, 256), BF16),
            pltpu.VMEM((model, width), BF16),
            pltpu.VMEM((2 * width, model), BF16),
            pltpu.VMEM((NZ, rows // BLOCK, BLOCK, 128), BF16),
            pltpu.VMEM((NZ * NY * rows // BLOCK, BLOCK, 128), BF16),
            pltpu.VMEM((NZ, rows // 2, 128), BF16),
            pltpu.VMEM((NZ, rows // 2, 128), BF16),
            pltpu.VMEM((8, 128), jnp.int32),
            pltpu.VMEM((NZ, 8, 128), jnp.int32),
            pltpu.SMEM((NZ, 8, 128), jnp.int32),
            pltpu.VMEM((rows // BLOCK, BLOCK, 128), BF16),
            pltpu.VMEM((rows // 2, 128), BF16),
            pltpu.VMEM((2, 2, BLOCK, PICKS * BLOCK), F32),
            pltpu.VMEM((NZ, 2, 128, 128), BF16),
            pltpu.VMEM((2 * NZ, 128, 128), BF16),
            pltpu.VMEM((128, 128), F32),
            pltpu.VMEM((NZ, 8, 128), F32),
            pltpu.VMEM((NZ, 8, 128), F32),
            pltpu.VMEM((rows // 2, 2 * width), BF16),
            dma((10,)), dma, dma, dma, dma((3,)), dma((2,)), dma,
            dma((NZ,)), dma((NZ,)), dma((NZ,)), dma((NZ,)), dma((NZ,)), dma((NZ,)),
            dma((2,)), dma((2,)), dma((NZ, 2)), dma((NZ, 2)), dma((NZ, 2)), dma((NZ, 2)),
            dma((NZ, 2)), dma((2 * NZ,)), dma((NZ,)), dma((NZ,)),
        ],
        compiler_params=pltpu.CompilerParams(collective_id=0, has_side_effects=True, vmem_limit_bytes=62 * 2**20),
        name="heads_over_z",
    )(tokens[0], w_query, w_key, w_value, w_out, chosen[0])
    return mixed[None], log_sums[None]


def solution(mesh):
    return jax.shard_map(
        on_device,
        mesh=mesh,
        in_specs=(
            P("dp", "kv", None),
            P(None, "tp"),
            P(None, "tp"),
            P(None, "tp"),
            P("tp", None),
            P("dp", "kv", None),
        ),
        out_specs=(P("dp", ("kv", "tp"), None), P("dp", "tp", "kv")),
        check_vma=False,
    )
```

```python
import functools

import jax
import jax.numpy as jnp
from jax import lax
from jax.experimental import pallas as pl
from jax.experimental.pallas import tpu as pltpu
from jax.sharding import PartitionSpec as P

HEAD_DIM = 64
BLOCK = 64
NZ = 8
NY = 4
PICKS = 16
LOG2E = 1.4426950408889634
MESH = pl.DeviceIdType.MESH
BF16 = jnp.bfloat16
F32 = jnp.float32


def arrival_order(step, me_z):
    distance = (step + 1) // 2
    onward = lax.rem(me_z + step, 2) == 1
    offset = jnp.where(onward, distance, NZ - distance)
    return lax.rem(me_z + offset, NZ)


def kernel(
    x_hbm, wq_hbm, wk_hbm, wv_hbm, wo_hbm, chosen_ref, out_ref, logs_ref,
    x, wkv, wq, wo, kvs, land, qs, qland, cs, cland, picks, scores, os, oland, stat, ls, lland, att,
    in_sem, wo_sem, wo_send, wo_recv, own_sem, own_out_sem, pick_sem,
    kv_send, kv_recv, q_send, q_recv, c_send, c_recv,
    y_send, y_recv, f_send, f_recv, o_send, o_recv, l_send, l_recv,
):
    kv = lax.axis_index("kv")
    core = lax.axis_index("tp")
    me_z, me_y = kv // NY, lax.rem(kv, NY)
    rows = x.shape[0]
    half = rows // 2
    blocks = rows // BLOCK
    up = me_z * NY + lax.rem(me_y + 1, NY)
    down = me_z * NY + lax.rem(me_y + NY - 1, NY)
    below = lax.rem(me_y + NY - 1, NY)
    above = lax.rem(me_y + 1, NY)

    def at(z):
        return z * NY + me_y

    barrier = pltpu.get_barrier_semaphore()
    for k in range(NZ):
        z = lax.rem(me_z + k, NZ)
        for c in range(2):
            if k == 0 and c == 0:
                pl.semaphore_signal(barrier, inc=1, device_id={"tp": 1 - core}, device_id_type=MESH)
            elif k > 0:
                pl.semaphore_signal(barrier, inc=1, device_id={"kv": at(z), "tp": c}, device_id_type=MESH)
    for peer in (up, down):
        pl.semaphore_signal(barrier, inc=1, device_id={"kv": peer}, device_id_type=MESH)

    x_copy = pltpu.make_async_copy(x_hbm, x, in_sem.at[0])
    x_copy.start()
    w_copies = []
    parity = lax.rem(me_z, 2)
    for n, turn in enumerate((0, 3 - 2 * parity, 1 + 2 * parity, 2)):
        pair = lax.rem(me_z // 2 + turn, NZ // 2)
        cols = pl.ds(pl.multiple_of(pair * 128, 128), 128)
        copies = []
        for i, src in enumerate((wk_hbm, wv_hbm)):
            copies.append(
                pltpu.make_async_copy(src.at[:, cols], wkv.at[n, :, pl.ds(i * 128, 128)], in_sem.at[1 + 2 * n + i])
            )
            if n == 0:
                copies[-1].start()
        w_copies.append((pair, copies))
    wq_copy = pltpu.make_async_copy(wq_hbm, wq, in_sem.at[9])

    cs[...] = jnp.zeros_like(cs)
    cs[:, 0:PICKS] = jnp.maximum(chosen_ref[...], 0)
    lane = lax.broadcasted_iota(jnp.int32, (rows, 128), 1)
    low = lane < HEAD_DIM

    far = lax.rem(me_z + NZ // 2, NZ)

    def kv_copy(z):
        return pltpu.make_async_remote_copy(
            src_ref=kvs.at[z], dst_ref=land.at[pl.ds(kv * blocks, blocks)], send_sem=kv_send.at[z],
            recv_sem=kv_recv.at[me_z], device_id={"kv": at(z)}, device_id_type=MESH,
        )

    def kv_arrival(z):
        return pltpu.make_async_remote_copy(
            src_ref=kvs.at[z], dst_ref=land.at[pl.ds(at(z) * blocks, blocks)], send_sem=kv_send.at[z],
            recv_sem=kv_recv.at[z], device_id={"kv": at(z)}, device_id_type=MESH,
        )

    def q_copy(z, src):
        return pltpu.make_async_remote_copy(
            src_ref=qs.at[z], dst_ref=qland.at[src], send_sem=q_send.at[z],
            recv_sem=q_recv.at[src], device_id={"kv": at(z)}, device_id_type=MESH,
        )

    def c_copy(z, src):
        return pltpu.make_async_remote_copy(
            src_ref=cs, dst_ref=cland.at[src], send_sem=c_send.at[z],
            recv_sem=c_recv.at[src], device_id={"kv": at(z)}, device_id_type=MESH,
        )

    def y_copy(z, way, src=None):
        rng = pl.ds(at(z) * blocks, blocks)
        return pltpu.make_async_remote_copy(
            src_ref=land.at[rng] if src is None else src, dst_ref=land.at[rng], send_sem=y_send.at[z, way],
            recv_sem=y_recv.at[z, way], device_id={"kv": (up, down)[way]}, device_id_type=MESH,
        )

    own_kv = pltpu.make_async_copy(kvs.at[me_z], land.at[pl.ds(kv * blocks, blocks)], own_sem.at[0])
    own_c = pltpu.make_async_copy(cs, cland.at[me_z], own_sem.at[1])
    x_copy.wait()
    for _, copies in w_copies[1:]:
        for c in copies:
            c.start()
    wq_copy.start()
    for n, (pair, copies) in enumerate(w_copies):
        for c in copies:
            c.wait()
        both = jnp.dot(x[...], wkv[n], preferred_element_type=F32)
        kp, vp = both[:, 0:128], both[:, 128:256]
        kvs[2 * pair] = jnp.where(low, kp, pltpu.roll(vp, HEAD_DIM, 1)).astype(BF16).reshape(blocks, BLOCK, 128)
        kvs[2 * pair + 1] = jnp.where(low, pltpu.roll(kp, HEAD_DIM, 1), vp).astype(BF16).reshape(blocks, BLOCK, 128)
        if n == 0:
            pl.semaphore_wait(barrier, 2 * NZ + 1)
            own_c.start()
            for t in range(1, NZ):
                c_copy(arrival_order(t, me_z), me_z).start()
            for way in range(2):
                y_copy(me_z, way, kvs.at[me_z]).start()
            own_kv.start()
            kv_copy(2 * pair + 1 - parity).start()
        elif n < 3:
            near = 1 - parity if n == 1 else parity
            kv_copy(2 * pair + near).start()
            kv_copy(2 * pair + 1 - near).start()
        else:
            kv_copy(far).start()
            kv_copy(2 * pair + 1 - parity).start()

    wo_rows = wo_hbm.shape[0]
    wo_mine = wo.at[pl.ds(core * wo_rows, wo_rows)]
    wo_local = pltpu.make_async_copy(wo_hbm, wo_mine, wo_sem)
    wo_local.start()
    wo_remote = pltpu.make_async_remote_copy(
        src_ref=wo_hbm, dst_ref=wo_mine, send_sem=wo_send, recv_sem=wo_recv,
        device_id={"tp": 1 - core}, device_id_type=MESH,
    )
    wo_remote.start()

    own_q = pltpu.make_async_copy(qs.at[me_z], qland.at[me_z], own_sem.at[2])

    def project_all_queries():
        wq_copy.wait()

        def project_queries(i, carry):
            res = jnp.dot(x[...], wq[:, pl.ds(pl.multiple_of(i * 256, 256), 256)], preferred_element_type=F32)
            lo = low[:half]
            for u in range(2):
                top, bot = res[:half, u * 128:(u + 1) * 128], res[half:, u * 128:(u + 1) * 128]
                qs[4 * i + 2 * u] = jnp.where(lo, top, pltpu.roll(bot, HEAD_DIM, 1)).astype(BF16)
                qs[4 * i + 2 * u + 1] = jnp.where(lo, pltpu.roll(top, HEAD_DIM, 1), bot).astype(BF16)
            return carry

        lax.fori_loop(0, 2, project_queries, 0)

    def send_queries():
        own_q.start()
        for t in range(7, 0, -1):
            q_copy(arrival_order(t, me_z), me_z).start()

    def y_arrival(z, way):
        rng = pl.ds((z * NY + (below, above)[way]) * blocks, blocks)
        return pltpu.make_async_remote_copy(
            src_ref=land.at[rng], dst_ref=land.at[rng], send_sem=y_send.at[z, way],
            recv_sem=y_recv.at[z, way], device_id={"kv": (up, down)[way]}, device_id_type=MESH,
        )

    def f_copy(z, way):
        rng = pl.ds((z * NY + (below, above)[way]) * blocks + way * (blocks // 2), blocks // 2)
        return pltpu.make_async_remote_copy(
            src_ref=land.at[rng], dst_ref=land.at[rng], send_sem=f_send.at[z, way],
            recv_sem=f_recv.at[z, way], device_id={"kv": (up, down)[way]}, device_id_type=MESH,
        )

    across = lax.rem(me_y + 2, NY)

    def f_arrival(z, way):
        rng = pl.ds((z * NY + across) * blocks + way * (blocks // 2), blocks // 2)
        return pltpu.make_async_remote_copy(
            src_ref=land.at[rng], dst_ref=land.at[rng], send_sem=f_send.at[z, way],
            recv_sem=f_recv.at[z, way], device_id={"kv": (up, down)[way]}, device_id_type=MESH,
        )

    own_kv.wait()
    for from_z, t in ((1, 1), (1, 2), (0, 0), (0, 1), (1, 3), (1, 4), (0, 2), (0, 3), (1, 5), (1, 6), (0, 4), (1, 7), (0, 5), (0, 6), (0, 7)):
        z = arrival_order(t, me_z)
        if from_z:
            kv_arrival(z).wait_recv()
            for way in range(2):
                y_copy(z, way).start()
        else:
            for way in range(2):
                y_arrival(z, way).wait_recv()
                f_copy(z, way).start()
        if (from_z, t) == (0, 1):
            project_all_queries()
        if (from_z, t) == (1, 7):
            send_queries()
    for z in range(NZ):
        for way in range(2):
            f_arrival(z, way).wait_recv()

    own_c.wait()
    own_q.wait()
    for t in range(1, NZ):
        z = arrival_order(t, me_z)
        c_copy(z, z).wait_recv()
    to_scalars = pltpu.make_async_copy(cland, picks, pick_sem)
    to_scalars.start()
    to_scalars.wait()

    lane_iota = lax.broadcasted_iota(jnp.int32, (128, 128), 1)
    low64 = lax.broadcasted_iota(jnp.int32, (BLOCK, 128), 1) < HEAD_DIM
    zero = jnp.zeros((BLOCK, 128), BF16)

    def o_copy(g, to):
        return pltpu.make_async_remote_copy(
            src_ref=os.at[g, to], dst_ref=oland.at[core * NZ + me_z], send_sem=o_send.at[g, to],
            recv_sem=o_recv.at[core * NZ + me_z], device_id={"kv": at(g), "tp": to}, device_id_type=MESH,
        )

    def l_copy(g, src):
        return pltpu.make_async_remote_copy(
            src_ref=ls.at[g], dst_ref=lland.at[src], send_sem=l_send.at[g],
            recv_sem=l_recv.at[src], device_id={"kv": at(g)}, device_id_type=MESH,
        )

    key_row = lax.broadcasted_iota(jnp.int32, (1, PICKS * BLOCK), 1)
    diagonal = jnp.where(
        lax.broadcasted_iota(jnp.int32, (BLOCK, 128), 1) >= BLOCK, 0.0,
        jnp.where(
            lax.broadcasted_iota(jnp.int32, (BLOCK, 128), 1) > lax.broadcasted_iota(jnp.int32, (BLOCK, 128), 0),
            -jnp.inf, 0.0,
        ),
    )

    def listed(g, j):
        return jnp.concatenate([land[picks[g, j, s]] for s in range(PICKS)], axis=0)

    def score(g, j, slot):
        tile = qland[g, j * BLOCK:(j + 1) * BLOCK, :].astype(F32)
        halves = (tile, pltpu.roll(tile, HEAD_DIM, 1))
        first, second = [jnp.where(low64, h, 0.0).astype(BF16) for h in halves]
        lhs = jnp.concatenate([jnp.concatenate([first, zero], axis=1), jnp.concatenate([zero, second], axis=1)], axis=0)
        keys = jnp.concatenate([listed(g, j), listed(g, j + 4)], axis=1)
        res = lax.dot_general(lhs, keys, (((1,), (1,)), ((), ())), preferred_element_type=F32)
        scores[slot, 0] = res[:BLOCK]
        scores[slot, 1] = res[BLOCK:]

    def finish(g, j, slot):
        device = g * NY + me_y
        for i in range(2):
            bias = jnp.where(key_row < (j + 4 * i + 2 * device + 1) * BLOCK, 0.0, -jnp.inf)
            s = scores[slot, i] + bias
            s = jnp.concatenate([s[:, 0:128] + diagonal, s[:, 128:]], axis=1)
            peak = jnp.max(s, axis=1, keepdims=True)
            e = jnp.exp2((s - peak) * (LOG2E * HEAD_DIM ** -0.5))
            total = jnp.sum(e, axis=1, keepdims=True)
            part = jnp.dot(e.astype(BF16), listed(g, j + 4 * i), preferred_element_type=F32) * (1.0 / total)
            log_sum = peak * HEAD_DIM ** -0.5 + jnp.log(total)
            band = slice(i * BLOCK, (i + 1) * BLOCK)
            stat[band, :] = jnp.where(lane_iota[band] == j, log_sum, stat[band, :])
            place = slice((j % 2) * BLOCK, (j % 2 + 1) * BLOCK)
            if j < 2:
                os[g, i, place, :] = pltpu.roll(part, HEAD_DIM, 1).astype(BF16)
            else:
                os[g, i, place, :] = jnp.where(low64, os[g, i, place, :].astype(F32), part).astype(BF16)

    def attend_group(t, carry):
        g = arrival_order(NZ - 1 - t, me_z)
        following = arrival_order(jnp.maximum(NZ - 2 - t, 0), me_z)

        @pl.when(t < NZ - 2)
        def _():
            q_copy(following, following).wait_recv()

        for j in range(4):
            if j < 3:
                score(g, j + 1, (j + 1) % 2)
            else:
                score(following, 0, 0)
            finish(g, j, j % 2)
        ls[g] = stat[...].T[0:8]

        @pl.when(g != me_z)
        def _():
            o_copy(g, 0).start()
            o_copy(g, 1).start()
            l_copy(g, me_z).start()

        @pl.when(g == me_z)
        def _():
            o_copy(g, 1 - core).start()
            pltpu.make_async_copy(os.at[g, core], oland.at[core * NZ + me_z], own_out_sem.at[0]).start()
            pltpu.make_async_copy(ls.at[g], lland.at[me_z], own_out_sem.at[1]).start()

        return carry

    stat[...] = jnp.zeros_like(stat)
    os[...] = jnp.zeros_like(os)
    q_copy(far, far).wait_recv()
    score(far, 0, 0)
    lax.fori_loop(0, NZ, attend_group, 0)

    def o_arrival(head):
        return pltpu.make_async_remote_copy(
            src_ref=os.at[0, 0], dst_ref=oland.at[head], send_sem=o_send.at[0, 0],
            recv_sem=o_recv.at[head], device_id={"tp": 1 - core}, device_id_type=MESH,
        )

    pltpu.make_async_copy(os.at[me_z, core], oland.at[core * NZ + me_z], own_out_sem.at[0]).wait()
    pltpu.make_async_copy(ls.at[me_z], lland.at[me_z], own_out_sem.at[1]).wait()
    for t in range(1, NZ):
        z = arrival_order(t, me_z)
        o_arrival(core * NZ + z).wait_recv()
        l_copy(z, z).wait_recv()
    for z in range(NZ):
        o_arrival((1 - core) * NZ + z).wait_recv()
    low128 = lane_iota < HEAD_DIM
    for i in range(NZ):
        a, b = oland[2 * i].astype(F32), oland[2 * i + 1].astype(F32)
        cols = pl.ds(i * 128, 128)
        att[0:128, cols] = jnp.where(low128, a, pltpu.roll(b, HEAD_DIM, 1)).astype(BF16)
        att[128:256, cols] = jnp.where(low128, pltpu.roll(a, HEAD_DIM, 1), b).astype(BF16)
    low8 = low128[:8]
    for h in range(NZ):
        mine = lland[h]
        turned = pltpu.roll(mine, HEAD_DIM, 1)
        for q, (one, other) in enumerate(
            ((mine[0:1], turned[1:2]), (mine[2:3], turned[3:4]), (turned[0:1], mine[1:2]), (turned[2:3], mine[3:4]))
        ):
            logs_ref[h:h + 1, q * 128:(q + 1) * 128] = jnp.where(low8[:1], one, other)
    wo_local.wait()
    wo_remote.wait_send()
    pltpu.make_async_remote_copy(
        src_ref=wo_hbm, dst_ref=wo.at[pl.ds((1 - core) * wo_rows, wo_rows)], send_sem=wo_send, recv_sem=wo_recv,
        device_id={"tp": 1 - core}, device_id_type=MESH,
    ).wait_recv()

    def project_out(n, carry):
        cols = pl.ds(pl.multiple_of(n * 512, 512), 512)
        out_ref[:, cols] = jnp.dot(att[...], wo[:, cols], preferred_element_type=F32).astype(BF16)
        return carry

    lax.fori_loop(0, out_ref.shape[1] // 512, project_out, 0)

    for t in range(1, NZ):
        z = arrival_order(t, me_z)
        kv_copy(z).wait_send()
        q_copy(z, me_z).wait_send()
        c_copy(z, me_z).wait_send()
        o_copy(z, 0).wait_send()
        o_copy(z, 1).wait_send()
        l_copy(z, me_z).wait_send()
    o_copy(me_z, 1 - core).wait_send()

    for z in range(NZ):
        for way in range(2):
            y_copy(z, way).wait_send()
            f_copy(z, way).wait_send()


def on_device(tokens, w_query, w_key, w_value, w_out, chosen):
    rows, model = tokens.shape[1:]
    width = w_query.shape[1]
    hbm = pl.BlockSpec(memory_space=pl.ANY)
    vmem = pl.BlockSpec(memory_space=pltpu.VMEM)
    dma = pltpu.SemaphoreType.DMA
    mixed, log_sums = pl.pallas_call(
        kernel,
        out_shape=(
            jax.ShapeDtypeStruct((rows // 2, model), BF16),
            jax.ShapeDtypeStruct((width // HEAD_DIM, rows), F32),
        ),
        in_specs=[hbm] * 5 + [vmem],
        out_specs=(vmem, vmem),
        scratch_shapes=[
            pltpu.VMEM((rows, model), BF16),
            pltpu.VMEM((4, model, 256), BF16),
            pltpu.VMEM((model, width), BF16),
            pltpu.VMEM((2 * width, model), BF16),
            pltpu.VMEM((NZ, rows // BLOCK, BLOCK, 128), BF16),
            pltpu.VMEM((NZ * NY * rows // BLOCK, BLOCK, 128), BF16),
            pltpu.VMEM((NZ, rows // 2, 128), BF16),
            pltpu.VMEM((NZ, rows // 2, 128), BF16),
            pltpu.VMEM((8, 128), jnp.int32),
            pltpu.VMEM((NZ, 8, 128), jnp.int32),
            pltpu.SMEM((NZ, 8, 128), jnp.int32),
            pltpu.VMEM((2, 2, BLOCK, PICKS * BLOCK), F32),
            pltpu.VMEM((NZ, 2, 128, 128), BF16),
            pltpu.VMEM((2 * NZ, 128, 128), BF16),
            pltpu.VMEM((128, 128), F32),
            pltpu.VMEM((NZ, 8, 128), F32),
            pltpu.VMEM((NZ, 8, 128), F32),
            pltpu.VMEM((rows // 2, 2 * width), BF16),
            dma((10,)), dma, dma, dma, dma((3,)), dma((2,)), dma,
            dma((NZ,)), dma((NZ,)), dma((NZ,)), dma((NZ,)), dma((NZ,)), dma((NZ,)),
            dma((NZ, 2)), dma((NZ, 2)), dma((NZ, 2)), dma((NZ, 2)),
            dma((NZ, 2)), dma((2 * NZ,)), dma((NZ,)), dma((NZ,)),
        ],
        compiler_params=pltpu.CompilerParams(collective_id=0, has_side_effects=True, vmem_limit_bytes=52 * 2**20),
        name="heads_over_z",
    )(tokens[0], w_query, w_key, w_value, w_out, chosen[0])
    return mixed[None], log_sums[None]


def solution(mesh):
    return jax.shard_map(
        on_device,
        mesh=mesh,
        in_specs=(
            P("dp", "kv", None),
            P(None, "tp"),
            P(None, "tp"),
            P(None, "tp"),
            P("tp", None),
            P("dp", "kv", None),
        ),
        out_specs=(P("dp", ("kv", "tp"), None), P("dp", "tp", "kv")),
        check_vma=False,
    )
```

```python
import functools

import jax
import jax.numpy as jnp
from jax import lax
from jax.experimental import pallas as pl
from jax.experimental.pallas import tpu as pltpu
from jax.sharding import PartitionSpec as P

HEAD_DIM = 64
BLOCK = 64
NZ = 8
NY = 4
EVENTS = (
    (1, 1), (1, 2), (0, 0), (0, 1), (1, 3), (1, 4), (0, 2), (0, 3), (1, 5), (0, 4), (1, 6), (1, 7), (0, 5), (0, 6),
)
PICKS = 16
EARLY = 3
LOG2E = 1.4426950408889634
MESH = pl.DeviceIdType.MESH
BF16 = jnp.bfloat16
F32 = jnp.float32


def arrival_order(step, me_z):
    distance = (step + 1) // 2
    onward = lax.rem(me_z + step, 2) == 1
    offset = jnp.where(onward, distance, NZ - distance)
    return lax.rem(me_z + offset, NZ)


def gather_table():
    table = []
    for z in range(NZ):
        sign = 1 if z % 2 == 0 else -1
        offsets = [0, sign, -sign, 2 * sign, -2 * sign, 3 * sign, -3 * sign, 4]
        last = {4: 7, 5: 7, 6: 3}.get(z, (z + 4) % NZ)
        found = [(z + o) % NZ for o in offsets]
        found.remove(last)
        table.append(found + [last])
    return table


def group_table():
    table = []
    for z in range(NZ):
        last = gather_table()[z][-1]
        far_first = sorted((g for g in range(NZ) if g != z), key=lambda g: -min((g - z) % NZ, (z - g) % NZ))
        early = [g for g in far_first if g < last][:EARLY]
        table.append(early + [g for g in far_first if g not in early] + [z])
    return table


def lookup(table, step, me_z):
    value = table[0][step]
    for z in range(1, NZ):
        value = jnp.where(me_z == z, table[z][step], value)
    return value


def kernel(
    x_hbm, wq_hbm, wk_hbm, wv_hbm, wo_hbm, chosen_hbm, out_ref, logs_ref,
    x, wkv, wq, wo, kvs, land, late, listing, qs, qland, cs, cland, picks, scores, os, oland, stat, ls, lland, att,
    in_sem, wo_sem, wo_send, wo_recv, own_sem, own_out_sem, pick_sem,
    kv_send, kv_recv, q_send, q_recv, c_send, c_recv,
    y_send, y_recv, f_send, f_recv, o_send, o_recv, l_send, l_recv,
):
    kv = lax.axis_index("kv")
    core = lax.axis_index("tp")
    me_z, me_y = kv // NY, lax.rem(kv, NY)
    rows = x.shape[0]
    half = rows // 2
    blocks = rows // BLOCK
    up = me_z * NY + lax.rem(me_y + 1, NY)
    down = me_z * NY + lax.rem(me_y + NY - 1, NY)
    below = lax.rem(me_y + NY - 1, NY)
    above = lax.rem(me_y + 1, NY)

    def at(z):
        return z * NY + me_y

    gather_order = [lookup(gather_table(), t, me_z) for t in range(NZ)]
    group_order = [lookup(group_table(), t, me_z) for t in range(NZ)]
    last_z = gather_order[-1]

    barrier = pltpu.get_barrier_semaphore()
    for k in range(NZ):
        z = lax.rem(me_z + k, NZ)
        for c in range(2):
            if k == 0 and c == 0:
                pl.semaphore_signal(barrier, inc=1, device_id={"tp": 1 - core}, device_id_type=MESH)
            elif k > 0:
                pl.semaphore_signal(barrier, inc=1, device_id={"kv": at(z), "tp": c}, device_id_type=MESH)
    for peer in (up, down):
        pl.semaphore_signal(barrier, inc=1, device_id={"kv": peer}, device_id_type=MESH)

    x_copy = pltpu.make_async_copy(x_hbm, x, in_sem.at[0])
    x_copy.start()
    list_copy = pltpu.make_async_copy(chosen_hbm, listing, pick_sem)
    list_copy.start()
    w_copies = []
    parity = lax.rem(me_z, 2)
    for n, turn in enumerate((0, 3 - 2 * parity, 1 + 2 * parity, 2)):
        pair = lax.rem(me_z // 2 + turn, NZ // 2)
        cols = pl.ds(pl.multiple_of(pair * 128, 128), 128)
        copies = []
        for i, src in enumerate((wk_hbm, wv_hbm)):
            copies.append(
                pltpu.make_async_copy(src.at[:, cols], wkv.at[n, :, pl.ds(i * 128, 128)], in_sem.at[1 + 2 * n + i])
            )
            if n == 0:
                copies[-1].start()
        w_copies.append((pair, copies))
    wq_copy = pltpu.make_async_copy(wq_hbm, wq, in_sem.at[9])

    cs[...] = jnp.zeros_like(cs)
    list_copy.wait()
    cs[:, 0:PICKS] = jnp.maximum(listing[...], 0)
    lane = lax.broadcasted_iota(jnp.int32, (rows, 128), 1)
    low = lane < HEAD_DIM

    far = lax.rem(me_z + NZ // 2, NZ)

    def kv_copy(z):
        return pltpu.make_async_remote_copy(
            src_ref=kvs.at[z], dst_ref=land.at[pl.ds(kv * blocks, blocks)], send_sem=kv_send.at[z],
            recv_sem=kv_recv.at[me_z], device_id={"kv": at(z)}, device_id_type=MESH,
        )

    def kv_arrival(z):
        return pltpu.make_async_remote_copy(
            src_ref=kvs.at[z], dst_ref=land.at[pl.ds(at(z) * blocks, blocks)], send_sem=kv_send.at[z],
            recv_sem=kv_recv.at[z], device_id={"kv": at(z)}, device_id_type=MESH,
        )

    def q_copy(z, src):
        return pltpu.make_async_remote_copy(
            src_ref=qs.at[z], dst_ref=qland.at[src], send_sem=q_send.at[z],
            recv_sem=q_recv.at[src], device_id={"kv": at(z)}, device_id_type=MESH,
        )

    def c_copy(z, src):
        return pltpu.make_async_remote_copy(
            src_ref=cs, dst_ref=cland.at[src], send_sem=c_send.at[z],
            recv_sem=c_recv.at[src], device_id={"kv": at(z)}, device_id_type=MESH,
        )

    def y_copy(z, way, src=None):
        rng = pl.ds(at(z) * blocks, blocks)
        return pltpu.make_async_remote_copy(
            src_ref=land.at[rng] if src is None else src, dst_ref=land.at[rng], send_sem=y_send.at[z, way],
            recv_sem=y_recv.at[z, way], device_id={"kv": (up, down)[way]}, device_id_type=MESH,
        )

    own_kv = pltpu.make_async_copy(kvs.at[me_z], land.at[pl.ds(kv * blocks, blocks)], own_sem.at[0])
    own_c = pltpu.make_async_copy(cs, cland.at[me_z], own_sem.at[1])
    x_copy.wait()
    for _, copies in w_copies[1:]:
        for c in copies:
            c.start()
    wq_copy.start()
    for n, (pair, copies) in enumerate(w_copies):
        for c in copies:
            c.wait()
        both = jnp.dot(x[...], wkv[n], preferred_element_type=F32)
        kp, vp = both[:, 0:128], both[:, 128:256]
        kvs[2 * pair] = jnp.where(low, kp, pltpu.roll(vp, HEAD_DIM, 1)).astype(BF16).reshape(blocks, BLOCK, 128)
        kvs[2 * pair + 1] = jnp.where(low, pltpu.roll(kp, HEAD_DIM, 1), vp).astype(BF16).reshape(blocks, BLOCK, 128)
        if n == 0:
            pl.semaphore_wait(barrier, 2 * NZ + 1)
            own_c.start()
            for t in range(1, NZ):
                c_copy(arrival_order(t, me_z), me_z).start()
            for way in range(2):
                y_copy(me_z, way, kvs.at[me_z]).start()
            own_kv.start()
            kv_copy(2 * pair + 1 - parity).start()
        elif n < 3:
            near = 1 - parity if n == 1 else parity
            kv_copy(2 * pair + near).start()
            kv_copy(2 * pair + 1 - near).start()
        else:
            kv_copy(far).start()
            kv_copy(2 * pair + 1 - parity).start()

    wo_rows = wo_hbm.shape[0]
    wo_mine = wo.at[pl.ds(core * wo_rows, wo_rows)]
    wo_local = pltpu.make_async_copy(wo_hbm, wo_mine, wo_sem)
    wo_remote = pltpu.make_async_remote_copy(
        src_ref=wo_hbm, dst_ref=wo_mine, send_sem=wo_send, recv_sem=wo_recv,
        device_id={"tp": 1 - core}, device_id_type=MESH,
    )

    own_q = pltpu.make_async_copy(qs.at[me_z], qland.at[me_z], own_sem.at[2])

    def project_all_queries():
        wq_copy.wait()

        def project_queries(i, carry):
            res = jnp.dot(x[...], wq[:, pl.ds(pl.multiple_of(i * 256, 256), 256)], preferred_element_type=F32)
            lo = low[:half]
            for u in range(2):
                top, bot = res[:half, u * 128:(u + 1) * 128], res[half:, u * 128:(u + 1) * 128]
                qs[4 * i + 2 * u] = jnp.where(lo, top, pltpu.roll(bot, HEAD_DIM, 1)).astype(BF16)
                qs[4 * i + 2 * u + 1] = jnp.where(lo, pltpu.roll(top, HEAD_DIM, 1), bot).astype(BF16)
            return carry

        lax.fori_loop(0, 2, project_queries, 0)

    def send_queries():
        own_q.start()
        for t in range(7, 0, -1):
            q_copy(arrival_order(t, me_z), me_z).start()

    def late_copy(way):
        rng = pl.ds(me_y * blocks, blocks)
        return pltpu.make_async_remote_copy(
            src_ref=land.at[pl.ds(at(last_z) * blocks, blocks)], dst_ref=late.at[rng], send_sem=y_send.at[last_z, way],
            recv_sem=y_recv.at[last_z, way], device_id={"kv": (up, down)[way]}, device_id_type=MESH,
        )

    def arrived(buffer, first, count, sems, z, way):
        rng = pl.ds(first, count)
        return pltpu.make_async_remote_copy(
            src_ref=buffer.at[rng], dst_ref=buffer.at[rng], send_sem=sems[0].at[z, way],
            recv_sem=sems[1].at[z, way], device_id={"kv": (up, down)[way]}, device_id_type=MESH,
        )

    across = lax.rem(me_y + 2, NY)

    def base(z, late_one):
        return 0 if late_one else z * NY * blocks

    def y_arrival(z, way, late_one=False):
        first = base(z, late_one) + (below, above)[way] * blocks
        return arrived(late if late_one else land, first, blocks, (y_send, y_recv), z, way)

    def f_copy(z, way, late_one=False):
        first = base(z, late_one) + (below, above)[way] * blocks + way * (blocks // 2)
        return arrived(late if late_one else land, first, blocks // 2, (f_send, f_recv), z, way)

    def f_arrival(z, way, late_one=False):
        first = base(z, late_one) + across * blocks + way * (blocks // 2)
        return arrived(late if late_one else land, first, blocks // 2, (f_send, f_recv), z, way)

    to_scalars = pltpu.make_async_copy(cland, picks, pick_sem)
    own_kv.wait()
    for from_z, t in EVENTS:
        z = gather_order[t]
        if from_z:
            kv_arrival(z).wait_recv()
            for way in range(2):
                (y_copy(z, way) if t < NZ - 1 else late_copy(way)).start()
        else:
            for way in range(2):
                y_arrival(z, way).wait_recv()
                f_copy(z, way).start()
        if (from_z, t) == (0, 1):
            project_all_queries()
            stat[...] = jnp.zeros_like(stat)
        if (from_z, t) == (0, 4):
            wo_local.start()
            wo_remote.start()
        if (from_z, t) == (0, 3):
            own_c.wait()
            for k in range(1, NZ):
                src = arrival_order(k, me_z)
                c_copy(src, src).wait_recv()
            to_scalars.start()
        if (from_z, t) == (1, NZ - 2):
            send_queries()
    for t in range(NZ - 1):
        for way in range(2):
            f_arrival(gather_order[t], way).wait_recv()

    own_q.wait()
    to_scalars.wait()

    lane_iota = lax.broadcasted_iota(jnp.int32, (128, 128), 1)
    low64 = lax.broadcasted_iota(jnp.int32, (BLOCK, 128), 1) < HEAD_DIM
    zero = jnp.zeros((BLOCK, 128), BF16)

    def o_copy(g, to):
        return pltpu.make_async_remote_copy(
            src_ref=os.at[g, to], dst_ref=oland.at[core * NZ + me_z], send_sem=o_send.at[g, to],
            recv_sem=o_recv.at[core * NZ + me_z], device_id={"kv": at(g), "tp": to}, device_id_type=MESH,
        )

    def l_copy(g, src):
        return pltpu.make_async_remote_copy(
            src_ref=ls.at[g], dst_ref=lland.at[src], send_sem=l_send.at[g],
            recv_sem=l_recv.at[src], device_id={"kv": at(g)}, device_id_type=MESH,
        )

    key_row = lax.broadcasted_iota(jnp.int32, (1, PICKS * BLOCK), 1)
    diagonal = jnp.where(
        lax.broadcasted_iota(jnp.int32, (BLOCK, 128), 1) >= BLOCK, 0.0,
        jnp.where(
            lax.broadcasted_iota(jnp.int32, (BLOCK, 128), 1) > lax.broadcasted_iota(jnp.int32, (BLOCK, 128), 0),
            -jnp.inf, 0.0,
        ),
    )

    def listed(g, j):
        return jnp.concatenate([land[picks[g, j, s]] for s in range(PICKS)], axis=0)

    def score(g, j, slot):
        tile = qland[g, j * BLOCK:(j + 1) * BLOCK, :].astype(F32)
        halves = (tile, pltpu.roll(tile, HEAD_DIM, 1))
        first, second = [jnp.where(low64, h, 0.0).astype(BF16) for h in halves]
        lhs = jnp.concatenate([jnp.concatenate([first, zero], axis=1), jnp.concatenate([zero, second], axis=1)], axis=0)
        keys = jnp.concatenate([listed(g, j), listed(g, j + 4)], axis=1)
        res = lax.dot_general(lhs, keys, (((1,), (1,)), ((), ())), preferred_element_type=F32)
        scores[slot, 0] = res[:BLOCK]
        scores[slot, 1] = res[BLOCK:]

    def finish(g, j, slot):
        device = g * NY + me_y
        exps, totals = [], []
        for i in range(2):
            bias = jnp.where(key_row < (j + 4 * i + 2 * device + 1) * BLOCK, 0.0, -jnp.inf)
            s = scores[slot, i] + bias
            s = jnp.concatenate([s[:, 0:128] + diagonal, s[:, 128:]], axis=1)
            peak = jnp.max(s, axis=1, keepdims=True)
            e = jnp.exp2((s - peak) * (LOG2E * HEAD_DIM ** -0.5))
            total = jnp.sum(e, axis=1, keepdims=True)
            log_sum = peak * HEAD_DIM ** -0.5 + jnp.log(total)
            band = slice(i * BLOCK, (i + 1) * BLOCK)
            stat[band, :] = jnp.where(lane_iota[band] == j, log_sum, stat[band, :])
            exps.append(e.astype(BF16))
            totals.append(total)
        values = jnp.concatenate([listed(g, j), listed(g, j + 4)], axis=1)
        both = jnp.dot(jnp.concatenate(exps, axis=0), values, preferred_element_type=F32)
        for i in range(2):
            part = both[i * BLOCK:(i + 1) * BLOCK, i * 128:(i + 1) * 128] * (1.0 / totals[i])
            place = slice((j % 2) * BLOCK, (j % 2 + 1) * BLOCK)
            if j < 2:
                os[g, i, place, :] = pltpu.roll(part, HEAD_DIM, 1).astype(BF16)
            else:
                os[g, i, place, :] = jnp.where(low64, os[g, i, place, :].astype(F32), part).astype(BF16)

    def group(t):
        value = group_order[0]
        for k in range(1, NZ):
            value = jnp.where(t == k, group_order[k], value)
        return value

    def attend_group(t, carry):
        g = group(t)
        following = group(jnp.where(t == EARLY - 1, t, jnp.minimum(t + 1, NZ - 1)))

        @pl.when((t < NZ - 2) & (t != EARLY - 1))
        def _():
            q_copy(following, following).wait_recv()

        for j in range(4):
            if j < 3:
                score(g, j + 1, (j + 1) % 2)
            else:
                score(following, 0, 0)
            finish(g, j, j % 2)
        ls[g] = stat[...].T[0:4]

        @pl.when(g != me_z)
        def _():
            o_copy(g, 0).start()
            o_copy(g, 1).start()
            l_copy(g, me_z).start()

        @pl.when(g == me_z)
        def _():
            o_copy(g, 1 - core).start()
            pltpu.make_async_copy(os.at[g, core], oland.at[core * NZ + me_z], own_out_sem.at[0]).start()
            pltpu.make_async_copy(ls.at[g], lland.at[me_z], own_out_sem.at[1]).start()

        return carry

    q_copy(group_order[0], group_order[0]).wait_recv()
    score(group_order[0], 0, 0)
    lax.fori_loop(0, 1, attend_group, 0)
    for way in range(2):
        y_arrival(last_z, way, True).wait_recv()
        f_copy(last_z, way, True).start()
    lax.fori_loop(1, EARLY, attend_group, 0)
    for way in range(2):
        f_arrival(last_z, way, True).wait_recv()
    for k in range(1, NY):
        y = lax.rem(me_y + k, NY)
        land[pl.ds((last_z * NY + y) * blocks, blocks)] = late[pl.ds(y * blocks, blocks)]
    q_copy(group_order[EARLY], group_order[EARLY]).wait_recv()
    score(group_order[EARLY], 0, 0)
    lax.fori_loop(EARLY, NZ, attend_group, 0)

    def o_arrival(head):
        return pltpu.make_async_remote_copy(
            src_ref=os.at[0, 0], dst_ref=oland.at[head], send_sem=o_send.at[0, 0],
            recv_sem=o_recv.at[head], device_id={"tp": 1 - core}, device_id_type=MESH,
        )

    pltpu.make_async_copy(os.at[me_z, core], oland.at[core * NZ + me_z], own_out_sem.at[0]).wait()
    pltpu.make_async_copy(ls.at[me_z], lland.at[me_z], own_out_sem.at[1]).wait()
    for t in range(1, NZ):
        z = arrival_order(t, me_z)
        o_arrival(core * NZ + z).wait_recv()
        l_copy(z, z).wait_recv()
    for z in range(NZ):
        o_arrival((1 - core) * NZ + z).wait_recv()
    low128 = lane_iota < HEAD_DIM
    for i in range(NZ):
        a, b = oland[2 * i].astype(F32), oland[2 * i + 1].astype(F32)
        cols = pl.ds(i * 128, 128)
        att[0:128, cols] = jnp.where(low128, a, pltpu.roll(b, HEAD_DIM, 1)).astype(BF16)
        att[128:256, cols] = jnp.where(low128, pltpu.roll(a, HEAD_DIM, 1), b).astype(BF16)
    low8 = low128[:8]
    for h in range(NZ):
        mine = lland[h]
        turned = pltpu.roll(mine, HEAD_DIM, 1)
        for q, (one, other) in enumerate(
            ((mine[0:1], turned[1:2]), (mine[2:3], turned[3:4]), (turned[0:1], mine[1:2]), (turned[2:3], mine[3:4]))
        ):
            logs_ref[h:h + 1, q * 128:(q + 1) * 128] = jnp.where(low8[:1], one, other)
    wo_local.wait()
    wo_remote.wait_send()
    pltpu.make_async_remote_copy(
        src_ref=wo_hbm, dst_ref=wo.at[pl.ds((1 - core) * wo_rows, wo_rows)], send_sem=wo_send, recv_sem=wo_recv,
        device_id={"tp": 1 - core}, device_id_type=MESH,
    ).wait_recv()

    def project_out(n, carry):
        cols = pl.ds(pl.multiple_of(n * 512, 512), 512)
        out_ref[:, cols] = jnp.dot(att[...], wo[:, cols], preferred_element_type=F32).astype(BF16)
        return carry

    lax.fori_loop(0, out_ref.shape[1] // 512, project_out, 0)

    for t in range(1, NZ):
        z = arrival_order(t, me_z)
        kv_copy(z).wait_send()
        q_copy(z, me_z).wait_send()
        c_copy(z, me_z).wait_send()
        o_copy(z, 0).wait_send()
        o_copy(z, 1).wait_send()
        l_copy(z, me_z).wait_send()
    o_copy(me_z, 1 - core).wait_send()

    for z in range(NZ):
        for way in range(2):
            y_copy(z, way).wait_send()
            f_copy(z, way).wait_send()


def on_device(tokens, w_query, w_key, w_value, w_out, chosen):
    rows, model = tokens.shape[1:]
    width = w_query.shape[1]
    hbm = pl.BlockSpec(memory_space=pl.ANY)
    vmem = pl.BlockSpec(memory_space=pltpu.VMEM)
    dma = pltpu.SemaphoreType.DMA
    mixed, log_sums = pl.pallas_call(
        kernel,
        out_shape=(
            jax.ShapeDtypeStruct((rows // 2, model), BF16),
            jax.ShapeDtypeStruct((width // HEAD_DIM, rows), F32),
        ),
        in_specs=[hbm] * 6,
        out_specs=(vmem, vmem),
        scratch_shapes=[
            pltpu.VMEM((rows, model), BF16),
            pltpu.VMEM((4, model, 256), BF16),
            pltpu.VMEM((model, width), BF16),
            pltpu.VMEM((2 * width, model), BF16),
            pltpu.VMEM((NZ, rows // BLOCK, BLOCK, 128), BF16),
            pltpu.VMEM((NZ * NY * rows // BLOCK, BLOCK, 128), BF16),
            pltpu.VMEM((NY * rows // BLOCK, BLOCK, 128), BF16),
            pltpu.VMEM(chosen.shape[1:], jnp.int32),
            pltpu.VMEM((NZ, rows // 2, 128), BF16),
            pltpu.VMEM((NZ, rows // 2, 128), BF16),
            pltpu.VMEM((8, 128), jnp.int32),
            pltpu.VMEM((NZ, 8, 128), jnp.int32),
            pltpu.SMEM((NZ, 8, 128), jnp.int32),
            pltpu.VMEM((2, 2, BLOCK, PICKS * BLOCK), F32),
            pltpu.VMEM((NZ, 2, 128, 128), BF16),
            pltpu.VMEM((2 * NZ, 128, 128), BF16),
            pltpu.VMEM((128, 128), F32),
            pltpu.VMEM((NZ, 4, 128), F32),
            pltpu.VMEM((NZ, 4, 128), F32),
            pltpu.VMEM((rows // 2, 2 * width), BF16),
            dma((10,)), dma, dma, dma, dma((3,)), dma((2,)), dma,
            dma((NZ,)), dma((NZ,)), dma((NZ,)), dma((NZ,)), dma((NZ,)), dma((NZ,)),
            dma((NZ, 2)), dma((NZ, 2)), dma((NZ, 2)), dma((NZ, 2)),
            dma((NZ, 2)), dma((2 * NZ,)), dma((NZ,)), dma((NZ,)),
        ],
        compiler_params=pltpu.CompilerParams(collective_id=0, has_side_effects=True, vmem_limit_bytes=52 * 2**20),
        name="heads_over_z",
    )(tokens[0], w_query, w_key, w_value, w_out, chosen[0])
    return mixed[None], log_sums[None]


def solution(mesh):
    return jax.shard_map(
        on_device,
        mesh=mesh,
        in_specs=(
            P("dp", "kv", None),
            P(None, "tp"),
            P(None, "tp"),
            P(None, "tp"),
            P("tp", None),
            P("dp", "kv", None),
        ),
        out_specs=(P("dp", ("kv", "tp"), None), P("dp", "tp", "kv")),
        check_vma=False,
    )
```

```python
import functools

import jax
import jax.numpy as jnp
from jax import lax
from jax.experimental import pallas as pl
from jax.experimental.pallas import tpu as pltpu
from jax.sharding import PartitionSpec as P

HEAD_DIM = 64
BLOCK = 64
NZ = 8
NY = 4
EVENTS = (
    (1, 1), (1, 2), (0, 0), (0, 1), (1, 3), (1, 4), (0, 2), (0, 3), (1, 5), (1, 6), (0, 4), (1, 7), (0, 5), (0, 6),
)
PICKS = 16
EARLY = 3
LOG2E = 1.4426950408889634
MESH = pl.DeviceIdType.MESH
BF16 = jnp.bfloat16
F32 = jnp.float32


def arrival_order(step, me_z):
    distance = (step + 1) // 2
    onward = lax.rem(me_z + step, 2) == 1
    offset = jnp.where(onward, distance, NZ - distance)
    return lax.rem(me_z + offset, NZ)


def gather_table():
    table = []
    for z in range(NZ):
        sign = 1 if z % 2 == 0 else -1
        offsets = [0, sign, -sign, 2 * sign, -2 * sign, 3 * sign, -3 * sign, 4]
        last = {4: 7, 5: 7, 6: 3}.get(z, (z + 4) % NZ)
        found = [(z + o) % NZ for o in offsets]
        found.remove(last)
        table.append(found + [last])
    return table


def group_table():
    table = []
    for z in range(NZ):
        last = gather_table()[z][-1]
        far_first = sorted((g for g in range(NZ) if g != z), key=lambda g: -min((g - z) % NZ, (z - g) % NZ))
        early = [g for g in far_first if g < last][:EARLY]
        table.append(early + [g for g in far_first if g not in early] + [z])
    return table


def lookup(table, step, me_z):
    value = table[0][step]
    for z in range(1, NZ):
        value = jnp.where(me_z == z, table[z][step], value)
    return value


def kernel(
    x_hbm, wq_hbm, wk_hbm, wv_hbm, wo_hbm, chosen_hbm, out_ref, logs_ref,
    x, wkv, wq, wo, kvs, land, late, listing, qs, qland, cs, cland, picks, scores, os, oland, stat, ls, lland, att,
    in_sem, wo_sem, wo_send, wo_recv, own_sem, own_out_sem, pick_sem,
    kv_send, kv_recv, q_send, q_recv, c_send, c_recv,
    y_send, y_recv, f_send, f_recv, o_send, o_recv, l_send, l_recv,
):
    kv = lax.axis_index("kv")
    core = lax.axis_index("tp")
    me_z, me_y = kv // NY, lax.rem(kv, NY)
    rows = x.shape[0]
    half = rows // 2
    blocks = rows // BLOCK
    up = me_z * NY + lax.rem(me_y + 1, NY)
    down = me_z * NY + lax.rem(me_y + NY - 1, NY)
    below = lax.rem(me_y + NY - 1, NY)
    above = lax.rem(me_y + 1, NY)

    def at(z):
        return z * NY + me_y

    gather_order = [lookup(gather_table(), t, me_z) for t in range(NZ)]
    group_order = [lookup(group_table(), t, me_z) for t in range(NZ)]
    last_z = gather_order[-1]

    barrier = pltpu.get_barrier_semaphore()
    for k in range(NZ):
        z = lax.rem(me_z + k, NZ)
        for c in range(2):
            if k == 0 and c == 0:
                pl.semaphore_signal(barrier, inc=1, device_id={"tp": 1 - core}, device_id_type=MESH)
            elif k > 0:
                pl.semaphore_signal(barrier, inc=1, device_id={"kv": at(z), "tp": c}, device_id_type=MESH)
    for peer in (up, down):
        pl.semaphore_signal(barrier, inc=1, device_id={"kv": peer}, device_id_type=MESH)

    x_copy = pltpu.make_async_copy(x_hbm, x, in_sem.at[0])
    x_copy.start()
    list_copy = pltpu.make_async_copy(chosen_hbm, listing, pick_sem)
    list_copy.start()
    w_copies = []
    parity = lax.rem(me_z, 2)
    for n, turn in enumerate((0, 3 - 2 * parity, 1 + 2 * parity, 2)):
        pair = lax.rem(me_z // 2 + turn, NZ // 2)
        cols = pl.ds(pl.multiple_of(pair * 128, 128), 128)
        copies = []
        for i, src in enumerate((wk_hbm, wv_hbm)):
            copies.append(
                pltpu.make_async_copy(src.at[:, cols], wkv.at[n, :, pl.ds(i * 128, 128)], in_sem.at[1 + 2 * n + i])
            )
            if n == 0:
                copies[-1].start()
        w_copies.append((pair, copies))
    wq_copy = pltpu.make_async_copy(wq_hbm, wq, in_sem.at[9])

    cs[...] = jnp.zeros_like(cs)
    list_copy.wait()
    cs[:, 0:PICKS] = jnp.maximum(listing[...], 0)
    lane = lax.broadcasted_iota(jnp.int32, (rows, 128), 1)
    low = lane < HEAD_DIM

    far = lax.rem(me_z + NZ // 2, NZ)

    def kv_copy(z):
        return pltpu.make_async_remote_copy(
            src_ref=kvs.at[z], dst_ref=land.at[pl.ds(kv * blocks, blocks)], send_sem=kv_send.at[z],
            recv_sem=kv_recv.at[me_z], device_id={"kv": at(z)}, device_id_type=MESH,
        )

    def kv_arrival(z):
        return pltpu.make_async_remote_copy(
            src_ref=kvs.at[z], dst_ref=land.at[pl.ds(at(z) * blocks, blocks)], send_sem=kv_send.at[z],
            recv_sem=kv_recv.at[z], device_id={"kv": at(z)}, device_id_type=MESH,
        )

    def q_copy(z, src):
        return pltpu.make_async_remote_copy(
            src_ref=qs.at[z], dst_ref=qland.at[src], send_sem=q_send.at[z],
            recv_sem=q_recv.at[src], device_id={"kv": at(z)}, device_id_type=MESH,
        )

    def c_copy(z, src):
        return pltpu.make_async_remote_copy(
            src_ref=cs, dst_ref=cland.at[src], send_sem=c_send.at[z],
            recv_sem=c_recv.at[src], device_id={"kv": at(z)}, device_id_type=MESH,
        )

    def y_copy(z, way, src=None):
        rng = pl.ds(at(z) * blocks, blocks)
        return pltpu.make_async_remote_copy(
            src_ref=land.at[rng] if src is None else src, dst_ref=land.at[rng], send_sem=y_send.at[z, way],
            recv_sem=y_recv.at[z, way], device_id={"kv": (up, down)[way]}, device_id_type=MESH,
        )

    own_kv = pltpu.make_async_copy(kvs.at[me_z], land.at[pl.ds(kv * blocks, blocks)], own_sem.at[0])
    own_c = pltpu.make_async_copy(cs, cland.at[me_z], own_sem.at[1])
    x_copy.wait()
    for _, copies in w_copies[1:]:
        for c in copies:
            c.start()
    wq_copy.start()
    for n, (pair, copies) in enumerate(w_copies):
        for c in copies:
            c.wait()
        both = jnp.dot(x[...], wkv[n], preferred_element_type=F32)
        kp, vp = both[:, 0:128], both[:, 128:256]
        kvs[2 * pair] = jnp.where(low, kp, pltpu.roll(vp, HEAD_DIM, 1)).astype(BF16).reshape(blocks, BLOCK, 128)
        kvs[2 * pair + 1] = jnp.where(low, pltpu.roll(kp, HEAD_DIM, 1), vp).astype(BF16).reshape(blocks, BLOCK, 128)
        if n == 0:
            pl.semaphore_wait(barrier, 2 * NZ + 1)
            own_c.start()
            for t in range(1, NZ):
                c_copy(arrival_order(t, me_z), me_z).start()
            for way in range(2):
                y_copy(me_z, way, kvs.at[me_z]).start()
            own_kv.start()
            kv_copy(2 * pair + 1 - parity).start()
        elif n < 3:
            near = 1 - parity if n == 1 else parity
            kv_copy(2 * pair + near).start()
            kv_copy(2 * pair + 1 - near).start()
        else:
            kv_copy(far).start()
            kv_copy(2 * pair + 1 - parity).start()

    wo_rows = wo_hbm.shape[0]
    wo_mine = wo.at[pl.ds(core * wo_rows, wo_rows)]
    wo_local = pltpu.make_async_copy(wo_hbm, wo_mine, wo_sem)
    wo_remote = pltpu.make_async_remote_copy(
        src_ref=wo_hbm, dst_ref=wo_mine, send_sem=wo_send, recv_sem=wo_recv,
        device_id={"tp": 1 - core}, device_id_type=MESH,
    )

    own_q = pltpu.make_async_copy(qs.at[me_z], qland.at[me_z], own_sem.at[2])

    def project_all_queries():
        wq_copy.wait()

        def project_queries(i, carry):
            res = jnp.dot(x[...], wq[:, pl.ds(pl.multiple_of(i * 256, 256), 256)], preferred_element_type=F32)
            lo = low[:half]
            for u in range(2):
                top, bot = res[:half, u * 128:(u + 1) * 128], res[half:, u * 128:(u + 1) * 128]
                qs[4 * i + 2 * u] = jnp.where(lo, top, pltpu.roll(bot, HEAD_DIM, 1)).astype(BF16)
                qs[4 * i + 2 * u + 1] = jnp.where(lo, pltpu.roll(top, HEAD_DIM, 1), bot).astype(BF16)
            return carry

        lax.fori_loop(0, 2, project_queries, 0)

    def send_queries():
        own_q.start()
        for t in range(7, 0, -1):
            q_copy(arrival_order(t, me_z), me_z).start()

    def late_copy(way):
        rng = pl.ds(me_y * blocks, blocks)
        return pltpu.make_async_remote_copy(
            src_ref=land.at[pl.ds(at(last_z) * blocks, blocks)], dst_ref=late.at[rng], send_sem=y_send.at[last_z, way],
            recv_sem=y_recv.at[last_z, way], device_id={"kv": (up, down)[way]}, device_id_type=MESH,
        )

    def arrived(buffer, first, count, sems, z, way):
        rng = pl.ds(first, count)
        return pltpu.make_async_remote_copy(
            src_ref=buffer.at[rng], dst_ref=buffer.at[rng], send_sem=sems[0].at[z, way],
            recv_sem=sems[1].at[z, way], device_id={"kv": (up, down)[way]}, device_id_type=MESH,
        )

    across = lax.rem(me_y + 2, NY)

    def base(z, late_one):
        return 0 if late_one else z * NY * blocks

    def y_arrival(z, way, late_one=False):
        first = base(z, late_one) + (below, above)[way] * blocks
        return arrived(late if late_one else land, first, blocks, (y_send, y_recv), z, way)

    def f_copy(z, way, late_one=False):
        first = base(z, late_one) + (below, above)[way] * blocks + way * (blocks // 2)
        return arrived(late if late_one else land, first, blocks // 2, (f_send, f_recv), z, way)

    def f_arrival(z, way, late_one=False):
        first = base(z, late_one) + across * blocks + way * (blocks // 2)
        return arrived(late if late_one else land, first, blocks // 2, (f_send, f_recv), z, way)

    to_scalars = pltpu.make_async_copy(cland, picks, pick_sem)
    own_kv.wait()
    for from_z, t in EVENTS:
        z = gather_order[t]
        if from_z:
            kv_arrival(z).wait_recv()
            for way in range(2):
                (y_copy(z, way) if t < NZ - 1 else late_copy(way)).start()
        else:
            for way in range(2):
                y_arrival(z, way).wait_recv()
                f_copy(z, way).start()
        if (from_z, t) == (0, 1):
            project_all_queries()
            stat[...] = jnp.zeros_like(stat)
        if (from_z, t) == (0, 4):
            wo_local.start()
            wo_remote.start()
        if (from_z, t) == (0, 3):
            own_c.wait()
            for k in range(1, NZ):
                src = arrival_order(k, me_z)
                c_copy(src, src).wait_recv()
            to_scalars.start()
        if (from_z, t) == (1, NZ - 2):
            send_queries()
    for t in range(NZ - 1):
        for way in range(2):
            f_arrival(gather_order[t], way).wait_recv()

    own_q.wait()
    to_scalars.wait()

    lane_iota = lax.broadcasted_iota(jnp.int32, (128, 128), 1)
    low64 = lax.broadcasted_iota(jnp.int32, (BLOCK, 128), 1) < HEAD_DIM
    zero = jnp.zeros((BLOCK, 128), BF16)

    def o_copy(g, to):
        return pltpu.make_async_remote_copy(
            src_ref=os.at[g, to], dst_ref=oland.at[core * NZ + me_z], send_sem=o_send.at[g, to],
            recv_sem=o_recv.at[core * NZ + me_z], device_id={"kv": at(g), "tp": to}, device_id_type=MESH,
        )

    def l_copy(g, src):
        return pltpu.make_async_remote_copy(
            src_ref=ls.at[g], dst_ref=lland.at[src], send_sem=l_send.at[g],
            recv_sem=l_recv.at[src], device_id={"kv": at(g)}, device_id_type=MESH,
        )

    key_row = lax.broadcasted_iota(jnp.int32, (1, PICKS * BLOCK), 1)
    diagonal = jnp.where(
        lax.broadcasted_iota(jnp.int32, (BLOCK, 128), 1) >= BLOCK, 0.0,
        jnp.where(
            lax.broadcasted_iota(jnp.int32, (BLOCK, 128), 1) > lax.broadcasted_iota(jnp.int32, (BLOCK, 128), 0),
            -jnp.inf, 0.0,
        ),
    )

    def listed(g, j):
        return jnp.concatenate([land[picks[g, j, s]] for s in range(PICKS)], axis=0)

    def score(g, j, slot):
        tile = qland[g, j * BLOCK:(j + 1) * BLOCK, :].astype(F32)
        halves = (tile, pltpu.roll(tile, HEAD_DIM, 1))
        first, second = [jnp.where(low64, h, 0.0).astype(BF16) for h in halves]
        lhs = jnp.concatenate([jnp.concatenate([first, zero], axis=1), jnp.concatenate([zero, second], axis=1)], axis=0)
        keys = jnp.concatenate([listed(g, j), listed(g, j + 4)], axis=1)
        res = lax.dot_general(lhs, keys, (((1,), (1,)), ((), ())), preferred_element_type=F32)
        scores[slot, 0] = res[:BLOCK]
        scores[slot, 1] = res[BLOCK:]

    def finish(g, j, slot):
        device = g * NY + me_y
        exps, totals = [], []
        for i in range(2):
            bias = jnp.where(key_row < (j + 4 * i + 2 * device + 1) * BLOCK, 0.0, -jnp.inf)
            s = scores[slot, i] + bias
            s = jnp.concatenate([s[:, 0:128] + diagonal, s[:, 128:]], axis=1)
            peak = jnp.max(s, axis=1, keepdims=True)
            e = jnp.exp2((s - peak) * (LOG2E * HEAD_DIM ** -0.5))
            total = jnp.sum(e, axis=1, keepdims=True)
            log_sum = peak * HEAD_DIM ** -0.5 + jnp.log(total)
            band = slice(i * BLOCK, (i + 1) * BLOCK)
            stat[band, :] = jnp.where(lane_iota[band] == j, log_sum, stat[band, :])
            exps.append(e.astype(BF16))
            totals.append(total)
        values = jnp.concatenate([listed(g, j), listed(g, j + 4)], axis=1)
        both = jnp.dot(jnp.concatenate(exps, axis=0), values, preferred_element_type=F32)
        for i in range(2):
            part = both[i * BLOCK:(i + 1) * BLOCK, i * 128:(i + 1) * 128] * (1.0 / totals[i])
            place = slice((j % 2) * BLOCK, (j % 2 + 1) * BLOCK)
            if j < 2:
                os[g, i, place, :] = pltpu.roll(part, HEAD_DIM, 1).astype(BF16)
            else:
                os[g, i, place, :] = jnp.where(low64, os[g, i, place, :].astype(F32), part).astype(BF16)

    def group(t):
        value = group_order[0]
        for k in range(1, NZ):
            value = jnp.where(t == k, group_order[k], value)
        return value

    def attend_group(t, carry):
        g = group(t)
        following = group(jnp.where(t == EARLY - 1, t, jnp.minimum(t + 1, NZ - 1)))

        @pl.when((t < NZ - 2) & (t != EARLY - 1))
        def _():
            q_copy(following, following).wait_recv()

        for j in range(4):
            if j < 3:
                score(g, j + 1, (j + 1) % 2)
            else:
                score(following, 0, 0)
            finish(g, j, j % 2)
        ls[g] = stat[...].T[0:4]

        @pl.when(g != me_z)
        def _():
            o_copy(g, 0).start()
            o_copy(g, 1).start()
            l_copy(g, me_z).start()

        @pl.when(g == me_z)
        def _():
            o_copy(g, 1 - core).start()
            pltpu.make_async_copy(os.at[g, core], oland.at[core * NZ + me_z], own_out_sem.at[0]).start()
            pltpu.make_async_copy(ls.at[g], lland.at[me_z], own_out_sem.at[1]).start()

        return carry

    q_copy(group_order[0], group_order[0]).wait_recv()
    score(group_order[0], 0, 0)
    lax.fori_loop(0, 1, attend_group, 0)
    for way in range(2):
        y_arrival(last_z, way, True).wait_recv()
        f_copy(last_z, way, True).start()
    lax.fori_loop(1, EARLY, attend_group, 0)
    for way in range(2):
        f_arrival(last_z, way, True).wait_recv()
    for k in range(1, NY):
        y = lax.rem(me_y + k, NY)
        land[pl.ds((last_z * NY + y) * blocks, blocks)] = late[pl.ds(y * blocks, blocks)]
    q_copy(group_order[EARLY], group_order[EARLY]).wait_recv()
    score(group_order[EARLY], 0, 0)
    lax.fori_loop(EARLY, NZ, attend_group, 0)

    def o_arrival(head):
        return pltpu.make_async_remote_copy(
            src_ref=os.at[0, 0], dst_ref=oland.at[head], send_sem=o_send.at[0, 0],
            recv_sem=o_recv.at[head], device_id={"tp": 1 - core}, device_id_type=MESH,
        )

    pltpu.make_async_copy(os.at[me_z, core], oland.at[core * NZ + me_z], own_out_sem.at[0]).wait()
    pltpu.make_async_copy(ls.at[me_z], lland.at[me_z], own_out_sem.at[1]).wait()
    for t in range(1, NZ):
        z = arrival_order(t, me_z)
        o_arrival(core * NZ + z).wait_recv()
        l_copy(z, z).wait_recv()
    for z in range(NZ):
        o_arrival((1 - core) * NZ + z).wait_recv()
    low128 = lane_iota < HEAD_DIM
    for i in range(NZ):
        a, b = oland[2 * i].astype(F32), oland[2 * i + 1].astype(F32)
        cols = pl.ds(i * 128, 128)
        att[0:128, cols] = jnp.where(low128, a, pltpu.roll(b, HEAD_DIM, 1)).astype(BF16)
        att[128:256, cols] = jnp.where(low128, pltpu.roll(a, HEAD_DIM, 1), b).astype(BF16)
    low8 = low128[:8]
    for h in range(NZ):
        mine = lland[h]
        turned = pltpu.roll(mine, HEAD_DIM, 1)
        for q, (one, other) in enumerate(
            ((mine[0:1], turned[1:2]), (mine[2:3], turned[3:4]), (turned[0:1], mine[1:2]), (turned[2:3], mine[3:4]))
        ):
            logs_ref[h:h + 1, q * 128:(q + 1) * 128] = jnp.where(low8[:1], one, other)
    wo_local.wait()
    wo_remote.wait_send()
    pltpu.make_async_remote_copy(
        src_ref=wo_hbm, dst_ref=wo.at[pl.ds((1 - core) * wo_rows, wo_rows)], send_sem=wo_send, recv_sem=wo_recv,
        device_id={"tp": 1 - core}, device_id_type=MESH,
    ).wait_recv()

    def project_out(n, carry):
        cols = pl.ds(pl.multiple_of(n * 512, 512), 512)
        out_ref[:, cols] = jnp.dot(att[...], wo[:, cols], preferred_element_type=F32).astype(BF16)
        return carry

    lax.fori_loop(0, out_ref.shape[1] // 512, project_out, 0)

    for t in range(1, NZ):
        z = arrival_order(t, me_z)
        kv_copy(z).wait_send()
        q_copy(z, me_z).wait_send()
        c_copy(z, me_z).wait_send()
        o_copy(z, 0).wait_send()
        o_copy(z, 1).wait_send()
        l_copy(z, me_z).wait_send()
    o_copy(me_z, 1 - core).wait_send()

    for z in range(NZ):
        for way in range(2):
            y_copy(z, way).wait_send()
            f_copy(z, way).wait_send()


def on_device(tokens, w_query, w_key, w_value, w_out, chosen):
    rows, model = tokens.shape[1:]
    width = w_query.shape[1]
    hbm = pl.BlockSpec(memory_space=pl.ANY)
    vmem = pl.BlockSpec(memory_space=pltpu.VMEM)
    dma = pltpu.SemaphoreType.DMA
    mixed, log_sums = pl.pallas_call(
        kernel,
        out_shape=(
            jax.ShapeDtypeStruct((rows // 2, model), BF16),
            jax.ShapeDtypeStruct((width // HEAD_DIM, rows), F32),
        ),
        in_specs=[hbm] * 6,
        out_specs=(vmem, vmem),
        scratch_shapes=[
            pltpu.VMEM((rows, model), BF16),
            pltpu.VMEM((4, model, 256), BF16),
            pltpu.VMEM((model, width), BF16),
            pltpu.VMEM((2 * width, model), BF16),
            pltpu.VMEM((NZ, rows // BLOCK, BLOCK, 128), BF16),
            pltpu.VMEM((NZ * NY * rows // BLOCK, BLOCK, 128), BF16),
            pltpu.VMEM((NY * rows // BLOCK, BLOCK, 128), BF16),
            pltpu.VMEM(chosen.shape[1:], jnp.int32),
            pltpu.VMEM((NZ, rows // 2, 128), BF16),
            pltpu.VMEM((NZ, rows // 2, 128), BF16),
            pltpu.VMEM((8, 128), jnp.int32),
            pltpu.VMEM((NZ, 8, 128), jnp.int32),
            pltpu.SMEM((NZ, 8, 128), jnp.int32),
            pltpu.VMEM((2, 2, BLOCK, PICKS * BLOCK), F32),
            pltpu.VMEM((NZ, 2, 128, 128), BF16),
            pltpu.VMEM((2 * NZ, 128, 128), BF16),
            pltpu.VMEM((128, 128), F32),
            pltpu.VMEM((NZ, 4, 128), F32),
            pltpu.VMEM((NZ, 4, 128), F32),
            pltpu.VMEM((rows // 2, 2 * width), BF16),
            dma((10,)), dma, dma, dma, dma((3,)), dma((2,)), dma,
            dma((NZ,)), dma((NZ,)), dma((NZ,)), dma((NZ,)), dma((NZ,)), dma((NZ,)),
            dma((NZ, 2)), dma((NZ, 2)), dma((NZ, 2)), dma((NZ, 2)),
            dma((NZ, 2)), dma((2 * NZ,)), dma((NZ,)), dma((NZ,)),
        ],
        compiler_params=pltpu.CompilerParams(collective_id=0, has_side_effects=True, vmem_limit_bytes=52 * 2**20),
        name="heads_over_z",
    )(tokens[0], w_query, w_key, w_value, w_out, chosen[0])
    return mixed[None], log_sums[None]


def solution(mesh):
    return jax.shard_map(
        on_device,
        mesh=mesh,
        in_specs=(
            P("dp", "kv", None),
            P(None, "tp"),
            P(None, "tp"),
            P(None, "tp"),
            P("tp", None),
            P("dp", "kv", None),
        ),
        out_specs=(P("dp", ("kv", "tp"), None), P("dp", "tp", "kv")),
        check_vma=False,
    )
```

```python
import functools

import jax
import jax.numpy as jnp
from jax import lax
from jax.experimental import pallas as pl
from jax.experimental.pallas import tpu as pltpu
from jax.sharding import PartitionSpec as P

HEAD_DIM = 64
BLOCK = 64
NZ = 8
NY = 4
EVENTS = (
    (1, 1), (1, 2), (0, 0), (0, 1), (1, 3), (1, 4), (0, 2), (0, 3), (1, 5), (1, 6), (0, 4), (1, 7), (0, 5), (0, 6),
)
PICKS = 16
EARLY = 3
LOG2E = 1.4426950408889634
MESH = pl.DeviceIdType.MESH
BF16 = jnp.bfloat16
F32 = jnp.float32


def arrival_order(step, me_z):
    distance = (step + 1) // 2
    onward = lax.rem(me_z + step, 2) == 1
    offset = jnp.where(onward, distance, NZ - distance)
    return lax.rem(me_z + offset, NZ)


def gather_table():
    table = []
    for z in range(NZ):
        sign = 1 if z % 2 == 0 else -1
        offsets = [0, sign, -sign, 2 * sign, -2 * sign, 3 * sign, -3 * sign, 4]
        last = {4: 7, 5: 7, 6: 3}.get(z, (z + 4) % NZ)
        found = [(z + o) % NZ for o in offsets]
        found.remove(last)
        table.append(found + [last])
    return table


def group_table():
    table = []
    for z in range(NZ):
        last = gather_table()[z][-1]
        far_first = sorted((g for g in range(NZ) if g != z), key=lambda g: -min((g - z) % NZ, (z - g) % NZ))
        early = [g for g in far_first if g < last][:EARLY]
        table.append(early + [g for g in far_first if g not in early] + [z])
    return table


def lookup(table, step, me_z):
    value = table[0][step]
    for z in range(1, NZ):
        value = jnp.where(me_z == z, table[z][step], value)
    return value


def kernel(
    x_hbm, wq_hbm, wk_hbm, wv_hbm, wo_hbm, chosen_hbm, out_ref, logs_ref,
    x, wkv, wq, wo, kvs, land, late, listing, qs, qland, cs, cland, picks, scores, os, oland, stat, ls, lland, att,
    in_sem, wo_sem, wo_send, wo_recv, own_sem, own_out_sem, pick_sem,
    kv_send, kv_recv, q_send, q_recv, c_send, c_recv,
    y_send, y_recv, f_send, f_recv, o_send, o_recv, l_send, l_recv,
):
    kv = lax.axis_index("kv")
    core = lax.axis_index("tp")
    me_z, me_y = kv // NY, lax.rem(kv, NY)
    rows = x.shape[0]
    half = rows // 2
    blocks = rows // BLOCK
    up = me_z * NY + lax.rem(me_y + 1, NY)
    down = me_z * NY + lax.rem(me_y + NY - 1, NY)
    below = lax.rem(me_y + NY - 1, NY)
    above = lax.rem(me_y + 1, NY)

    def at(z):
        return z * NY + me_y

    gather_order = [lookup(gather_table(), t, me_z) for t in range(NZ)]
    group_order = [lookup(group_table(), t, me_z) for t in range(NZ)]
    last_z = gather_order[-1]

    barrier = pltpu.get_barrier_semaphore()
    for k in range(NZ):
        z = lax.rem(me_z + k, NZ)
        for c in range(2):
            if k == 0 and c == 0:
                pl.semaphore_signal(barrier, inc=1, device_id={"tp": 1 - core}, device_id_type=MESH)
            elif k > 0:
                pl.semaphore_signal(barrier, inc=1, device_id={"kv": at(z), "tp": c}, device_id_type=MESH)
    for peer in (up, down):
        pl.semaphore_signal(barrier, inc=1, device_id={"kv": peer}, device_id_type=MESH)

    x_copy = pltpu.make_async_copy(x_hbm, x, in_sem.at[0])
    x_copy.start()
    list_copy = pltpu.make_async_copy(chosen_hbm, listing, pick_sem)
    list_copy.start()
    w_copies = []
    parity = lax.rem(me_z, 2)
    for n, turn in enumerate((0, 3 - 2 * parity, 1 + 2 * parity, 2)):
        pair = lax.rem(me_z // 2 + turn, NZ // 2)
        cols = pl.ds(pl.multiple_of(pair * 128, 128), 128)
        copies = []
        for i, src in enumerate((wk_hbm, wv_hbm)):
            copies.append(
                pltpu.make_async_copy(src.at[:, cols], wkv.at[n, :, pl.ds(i * 128, 128)], in_sem.at[1 + 2 * n + i])
            )
            if n == 0:
                copies[-1].start()
        w_copies.append((pair, copies))
    wq_copy = pltpu.make_async_copy(wq_hbm, wq, in_sem.at[9])

    cs[...] = jnp.zeros_like(cs)
    list_copy.wait()
    cs[:, 0:PICKS] = jnp.maximum(listing[...], 0)
    lane = lax.broadcasted_iota(jnp.int32, (rows, 128), 1)
    low = lane < HEAD_DIM

    far = lax.rem(me_z + NZ // 2, NZ)

    def kv_copy(z):
        return pltpu.make_async_remote_copy(
            src_ref=kvs.at[z], dst_ref=land.at[pl.ds(kv * blocks, blocks)], send_sem=kv_send.at[z],
            recv_sem=kv_recv.at[me_z], device_id={"kv": at(z)}, device_id_type=MESH,
        )

    def kv_arrival(z):
        return pltpu.make_async_remote_copy(
            src_ref=kvs.at[z], dst_ref=land.at[pl.ds(at(z) * blocks, blocks)], send_sem=kv_send.at[z],
            recv_sem=kv_recv.at[z], device_id={"kv": at(z)}, device_id_type=MESH,
        )

    def q_copy(z, src):
        return pltpu.make_async_remote_copy(
            src_ref=qs.at[z], dst_ref=qland.at[src], send_sem=q_send.at[z],
            recv_sem=q_recv.at[src], device_id={"kv": at(z)}, device_id_type=MESH,
        )

    def c_copy(z, src):
        return pltpu.make_async_remote_copy(
            src_ref=cs, dst_ref=cland.at[src], send_sem=c_send.at[z],
            recv_sem=c_recv.at[src], device_id={"kv": at(z)}, device_id_type=MESH,
        )

    def y_copy(z, way, src=None):
        rng = pl.ds(at(z) * blocks, blocks)
        return pltpu.make_async_remote_copy(
            src_ref=land.at[rng] if src is None else src, dst_ref=land.at[rng], send_sem=y_send.at[z, way],
            recv_sem=y_recv.at[z, way], device_id={"kv": (up, down)[way]}, device_id_type=MESH,
        )

    own_kv = pltpu.make_async_copy(kvs.at[me_z], land.at[pl.ds(kv * blocks, blocks)], own_sem.at[0])
    own_c = pltpu.make_async_copy(cs, cland.at[me_z], own_sem.at[1])
    x_copy.wait()
    for _, copies in w_copies[1:]:
        for c in copies:
            c.start()
    wq_copy.start()
    for n, (pair, copies) in enumerate(w_copies):
        for c in copies:
            c.wait()
        both = jnp.dot(x[...], wkv[n], preferred_element_type=F32)
        kp, vp = both[:, 0:128], both[:, 128:256]
        kvs[2 * pair] = jnp.where(low, kp, pltpu.roll(vp, HEAD_DIM, 1)).astype(BF16).reshape(blocks, BLOCK, 128)
        kvs[2 * pair + 1] = jnp.where(low, pltpu.roll(kp, HEAD_DIM, 1), vp).astype(BF16).reshape(blocks, BLOCK, 128)
        if n == 0:
            pl.semaphore_wait(barrier, 2 * NZ + 1)
            own_c.start()
            for t in range(1, NZ):
                c_copy(arrival_order(t, me_z), me_z).start()
            for way in range(2):
                y_copy(me_z, way, kvs.at[me_z]).start()
            own_kv.start()
            kv_copy(2 * pair + 1 - parity).start()
        elif n < 3:
            near = 1 - parity if n == 1 else parity
            kv_copy(2 * pair + near).start()
            kv_copy(2 * pair + 1 - near).start()
        else:
            kv_copy(far).start()
            kv_copy(2 * pair + 1 - parity).start()

    wo_rows = wo_hbm.shape[0]
    wo_mine = wo.at[pl.ds(core * wo_rows, wo_rows)]
    wo_local = pltpu.make_async_copy(wo_hbm, wo_mine, wo_sem)
    wo_remote = pltpu.make_async_remote_copy(
        src_ref=wo_hbm, dst_ref=wo_mine, send_sem=wo_send, recv_sem=wo_recv,
        device_id={"tp": 1 - core}, device_id_type=MESH,
    )

    own_q = pltpu.make_async_copy(qs.at[me_z], qland.at[me_z], own_sem.at[2])

    def project_all_queries():
        wq_copy.wait()

        def project_queries(i, carry):
            res = jnp.dot(x[...], wq[:, pl.ds(pl.multiple_of(i * 256, 256), 256)], preferred_element_type=F32)
            lo = low[:half]
            for u in range(2):
                top, bot = res[:half, u * 128:(u + 1) * 128], res[half:, u * 128:(u + 1) * 128]
                qs[4 * i + 2 * u] = jnp.where(lo, top, pltpu.roll(bot, HEAD_DIM, 1)).astype(BF16)
                qs[4 * i + 2 * u + 1] = jnp.where(lo, pltpu.roll(top, HEAD_DIM, 1), bot).astype(BF16)
            return carry

        lax.fori_loop(0, 2, project_queries, 0)

    def send_queries():
        own_q.start()
        for t in range(7, 0, -1):
            q_copy(arrival_order(t, me_z), me_z).start()

    def late_copy(way):
        rng = pl.ds(me_y * blocks, blocks)
        return pltpu.make_async_remote_copy(
            src_ref=land.at[pl.ds(at(last_z) * blocks, blocks)], dst_ref=late.at[rng], send_sem=y_send.at[last_z, way],
            recv_sem=y_recv.at[last_z, way], device_id={"kv": (up, down)[way]}, device_id_type=MESH,
        )

    def arrived(buffer, first, count, sems, z, way):
        rng = pl.ds(first, count)
        return pltpu.make_async_remote_copy(
            src_ref=buffer.at[rng], dst_ref=buffer.at[rng], send_sem=sems[0].at[z, way],
            recv_sem=sems[1].at[z, way], device_id={"kv": (up, down)[way]}, device_id_type=MESH,
        )

    across = lax.rem(me_y + 2, NY)

    def base(z, late_one):
        return 0 if late_one else z * NY * blocks

    def y_arrival(z, way, late_one=False):
        first = base(z, late_one) + (below, above)[way] * blocks
        return arrived(late if late_one else land, first, blocks, (y_send, y_recv), z, way)

    def f_copy(z, way, late_one=False):
        first = base(z, late_one) + (below, above)[way] * blocks + way * (blocks // 2)
        return arrived(late if late_one else land, first, blocks // 2, (f_send, f_recv), z, way)

    def f_arrival(z, way, late_one=False):
        first = base(z, late_one) + across * blocks + way * (blocks // 2)
        return arrived(late if late_one else land, first, blocks // 2, (f_send, f_recv), z, way)

    to_scalars = pltpu.make_async_copy(cland, picks, pick_sem)
    own_kv.wait()
    for from_z, t in EVENTS:
        z = gather_order[t]
        if from_z:
            kv_arrival(z).wait_recv()
            for way in range(2):
                (y_copy(z, way) if t < NZ - 1 else late_copy(way)).start()
        else:
            for way in range(2):
                y_arrival(z, way).wait_recv()
                f_copy(z, way).start()
        if (from_z, t) == (0, 1):
            project_all_queries()
            stat[...] = jnp.zeros_like(stat)
        if (from_z, t) == (0, 4):
            wo_local.start()
            wo_remote.start()
        if (from_z, t) == (0, 3):
            own_c.wait()
            for k in range(1, NZ):
                src = arrival_order(k, me_z)
                c_copy(src, src).wait_recv()
            to_scalars.start()
        if (from_z, t) == (1, NZ - 2):
            send_queries()
    for t in range(NZ - 1):
        for way in range(2):
            f_arrival(gather_order[t], way).wait_recv()

    own_q.wait()
    to_scalars.wait()

    lane_iota = lax.broadcasted_iota(jnp.int32, (128, 128), 1)
    low64 = lax.broadcasted_iota(jnp.int32, (BLOCK, 128), 1) < HEAD_DIM
    zero = jnp.zeros((BLOCK, 128), BF16)

    def o_copy(g, to):
        return pltpu.make_async_remote_copy(
            src_ref=os.at[g, to], dst_ref=oland.at[core * NZ + me_z], send_sem=o_send.at[g, to],
            recv_sem=o_recv.at[core * NZ + me_z], device_id={"kv": at(g), "tp": to}, device_id_type=MESH,
        )

    def l_copy(g, src):
        return pltpu.make_async_remote_copy(
            src_ref=ls.at[g], dst_ref=lland.at[src], send_sem=l_send.at[g],
            recv_sem=l_recv.at[src], device_id={"kv": at(g)}, device_id_type=MESH,
        )

    key_row = lax.broadcasted_iota(jnp.int32, (1, PICKS * BLOCK), 1)
    diagonal = jnp.where(
        lax.broadcasted_iota(jnp.int32, (BLOCK, 128), 1) >= BLOCK, 0.0,
        jnp.where(
            lax.broadcasted_iota(jnp.int32, (BLOCK, 128), 1) > lax.broadcasted_iota(jnp.int32, (BLOCK, 128), 0),
            -jnp.inf, 0.0,
        ),
    )

    def listed(g, j):
        return jnp.concatenate([land[picks[g, j, s]] for s in range(PICKS)], axis=0)

    def score(g, j, slot):
        tile = qland[g, j * BLOCK:(j + 1) * BLOCK, :].astype(F32)
        halves = (tile, pltpu.roll(tile, HEAD_DIM, 1))
        first, second = [jnp.where(low64, h, 0.0).astype(BF16) for h in halves]
        lhs = jnp.concatenate([jnp.concatenate([first, zero], axis=1), jnp.concatenate([zero, second], axis=1)], axis=0)
        keys = jnp.concatenate([listed(g, j), listed(g, j + 4)], axis=1)
        res = lax.dot_general(lhs, keys, (((1,), (1,)), ((), ())), preferred_element_type=F32)
        scores[slot, 0] = res[:BLOCK]
        scores[slot, 1] = res[BLOCK:]

    def finish(g, j, slot):
        device = g * NY + me_y
        exps, totals = [], []
        for i in range(2):
            bias = jnp.where(key_row < (j + 4 * i + 2 * device + 1) * BLOCK, 0.0, -jnp.inf)
            s = scores[slot, i] + bias
            s = jnp.concatenate([s[:, 0:128] + diagonal, s[:, 128:]], axis=1)
            peak = jnp.max(s, axis=1, keepdims=True)
            e = jnp.exp2((s - peak) * (LOG2E * HEAD_DIM ** -0.5))
            total = jnp.sum(e, axis=1, keepdims=True)
            log_sum = peak * HEAD_DIM ** -0.5 + jnp.log(total)
            band = slice(i * BLOCK, (i + 1) * BLOCK)
            stat[band, :] = jnp.where(lane_iota[band] == j, log_sum, stat[band, :])
            exps.append(e.astype(BF16))
            totals.append(total)
        values = jnp.concatenate([listed(g, j), listed(g, j + 4)], axis=1)
        both = jnp.dot(jnp.concatenate(exps, axis=0), values, preferred_element_type=F32)
        for i in range(2):
            part = both[i * BLOCK:(i + 1) * BLOCK, i * 128:(i + 1) * 128] * (1.0 / totals[i])
            place = slice((j % 2) * BLOCK, (j % 2 + 1) * BLOCK)
            if j < 2:
                os[g, i, place, :] = pltpu.roll(part, HEAD_DIM, 1).astype(BF16)
            else:
                os[g, i, place, :] = jnp.where(low64, os[g, i, place, :].astype(F32), part).astype(BF16)

    def group(t):
        value = group_order[0]
        for k in range(1, NZ):
            value = jnp.where(t == k, group_order[k], value)
        return value

    def attend_group(t, carry):
        g = group(t)
        following = group(jnp.where(t == EARLY - 1, t, jnp.minimum(t + 1, NZ - 1)))

        @pl.when((t < NZ - 2) & (t != EARLY - 1))
        def _():
            q_copy(following, following).wait_recv()

        for j in range(4):
            if j < 3:
                score(g, j + 1, (j + 1) % 2)
            else:
                score(following, 0, 0)
            finish(g, j, j % 2)
        ls[g] = stat[...].T[0:4]

        @pl.when(g != me_z)
        def _():
            o_copy(g, 0).start()
            o_copy(g, 1).start()
            l_copy(g, me_z).start()

        @pl.when(g == me_z)
        def _():
            o_copy(g, 1 - core).start()
            pltpu.make_async_copy(os.at[g, core], oland.at[core * NZ + me_z], own_out_sem.at[0]).start()
            pltpu.make_async_copy(ls.at[g], lland.at[me_z], own_out_sem.at[1]).start()

        return carry

    q_copy(group_order[0], group_order[0]).wait_recv()
    score(group_order[0], 0, 0)
    lax.fori_loop(0, 1, attend_group, 0)
    for way in range(2):
        y_arrival(last_z, way, True).wait_recv()
        f_copy(last_z, way, True).start()
    lax.fori_loop(1, EARLY, attend_group, 0)
    for way in range(2):
        f_arrival(last_z, way, True).wait_recv()
    for k in range(1, NY):
        y = lax.rem(me_y + k, NY)
        land[pl.ds((last_z * NY + y) * blocks, blocks)] = late[pl.ds(y * blocks, blocks)]
    q_copy(group_order[EARLY], group_order[EARLY]).wait_recv()
    score(group_order[EARLY], 0, 0)
    lax.fori_loop(EARLY, NZ, attend_group, 0)

    def o_arrival(head):
        return pltpu.make_async_remote_copy(
            src_ref=os.at[0, 0], dst_ref=oland.at[head], send_sem=o_send.at[0, 0],
            recv_sem=o_recv.at[head], device_id={"tp": 1 - core}, device_id_type=MESH,
        )

    pltpu.make_async_copy(os.at[me_z, core], oland.at[core * NZ + me_z], own_out_sem.at[0]).wait()
    pltpu.make_async_copy(ls.at[me_z], lland.at[me_z], own_out_sem.at[1]).wait()
    low128 = lane_iota < HEAD_DIM
    for turn in (2, 1, 3, 0):
        pair = lax.rem(me_z // 2 + turn, NZ // 2)
        for c in range(2):
            for m in range(2):
                z = 2 * pair + m

                @pl.when((z != me_z) | (core != c))
                def _():
                    o_arrival(c * NZ + z).wait_recv()

            a, b = oland[c * NZ + 2 * pair].astype(F32), oland[c * NZ + 2 * pair + 1].astype(F32)
            cols = pl.ds(pl.multiple_of((c * NZ // 2 + pair) * 128, 128), 128)
            att[0:128, cols] = jnp.where(low128, a, pltpu.roll(b, HEAD_DIM, 1)).astype(BF16)
            att[128:256, cols] = jnp.where(low128, pltpu.roll(a, HEAD_DIM, 1), b).astype(BF16)
    for t in range(1, NZ):
        z = arrival_order(t, me_z)
        l_copy(z, z).wait_recv()
    low8 = low128[:8]
    for h in range(NZ):
        mine = lland[h]
        turned = pltpu.roll(mine, HEAD_DIM, 1)
        for q, (one, other) in enumerate(
            ((mine[0:1], turned[1:2]), (mine[2:3], turned[3:4]), (turned[0:1], mine[1:2]), (turned[2:3], mine[3:4]))
        ):
            logs_ref[h:h + 1, q * 128:(q + 1) * 128] = jnp.where(low8[:1], one, other)
    wo_local.wait()
    wo_remote.wait_send()
    pltpu.make_async_remote_copy(
        src_ref=wo_hbm, dst_ref=wo.at[pl.ds((1 - core) * wo_rows, wo_rows)], send_sem=wo_send, recv_sem=wo_recv,
        device_id={"tp": 1 - core}, device_id_type=MESH,
    ).wait_recv()

    def project_out(n, carry):
        cols = pl.ds(pl.multiple_of(n * 512, 512), 512)
        out_ref[:, cols] = jnp.dot(att[...], wo[:, cols], preferred_element_type=F32).astype(BF16)
        return carry

    lax.fori_loop(0, out_ref.shape[1] // 512, project_out, 0)

    for t in range(1, NZ):
        z = arrival_order(t, me_z)
        kv_copy(z).wait_send()
        q_copy(z, me_z).wait_send()
        c_copy(z, me_z).wait_send()
        o_copy(z, 0).wait_send()
        o_copy(z, 1).wait_send()
        l_copy(z, me_z).wait_send()
    o_copy(me_z, 1 - core).wait_send()

    for z in range(NZ):
        for way in range(2):
            y_copy(z, way).wait_send()
            f_copy(z, way).wait_send()


def on_device(tokens, w_query, w_key, w_value, w_out, chosen):
    rows, model = tokens.shape[1:]
    width = w_query.shape[1]
    hbm = pl.BlockSpec(memory_space=pl.ANY)
    vmem = pl.BlockSpec(memory_space=pltpu.VMEM)
    dma = pltpu.SemaphoreType.DMA
    mixed, log_sums = pl.pallas_call(
        kernel,
        out_shape=(
            jax.ShapeDtypeStruct((rows // 2, model), BF16),
            jax.ShapeDtypeStruct((width // HEAD_DIM, rows), F32),
        ),
        in_specs=[hbm] * 6,
        out_specs=(vmem, vmem),
        scratch_shapes=[
            pltpu.VMEM((rows, model), BF16),
            pltpu.VMEM((4, model, 256), BF16),
            pltpu.VMEM((model, width), BF16),
            pltpu.VMEM((2 * width, model), BF16),
            pltpu.VMEM((NZ, rows // BLOCK, BLOCK, 128), BF16),
            pltpu.VMEM((NZ * NY * rows // BLOCK, BLOCK, 128), BF16),
            pltpu.VMEM((NY * rows // BLOCK, BLOCK, 128), BF16),
            pltpu.VMEM(chosen.shape[1:], jnp.int32),
            pltpu.VMEM((NZ, rows // 2, 128), BF16),
            pltpu.VMEM((NZ, rows // 2, 128), BF16),
            pltpu.VMEM((8, 128), jnp.int32),
            pltpu.VMEM((NZ, 8, 128), jnp.int32),
            pltpu.SMEM((NZ, 8, 128), jnp.int32),
            pltpu.VMEM((2, 2, BLOCK, PICKS * BLOCK), F32),
            pltpu.VMEM((NZ, 2, 128, 128), BF16),
            pltpu.VMEM((2 * NZ, 128, 128), BF16),
            pltpu.VMEM((128, 128), F32),
            pltpu.VMEM((NZ, 4, 128), F32),
            pltpu.VMEM((NZ, 4, 128), F32),
            pltpu.VMEM((rows // 2, 2 * width), BF16),
            dma((10,)), dma, dma, dma, dma((3,)), dma((2,)), dma,
            dma((NZ,)), dma((NZ,)), dma((NZ,)), dma((NZ,)), dma((NZ,)), dma((NZ,)),
            dma((NZ, 2)), dma((NZ, 2)), dma((NZ, 2)), dma((NZ, 2)),
            dma((NZ, 2)), dma((2 * NZ,)), dma((NZ,)), dma((NZ,)),
        ],
        compiler_params=pltpu.CompilerParams(collective_id=0, has_side_effects=True, vmem_limit_bytes=52 * 2**20),
        name="heads_over_z",
    )(tokens[0], w_query, w_key, w_value, w_out, chosen[0])
    return mixed[None], log_sums[None]


def solution(mesh):
    return jax.shard_map(
        on_device,
        mesh=mesh,
        in_specs=(
            P("dp", "kv", None),
            P(None, "tp"),
            P(None, "tp"),
            P(None, "tp"),
            P("tp", None),
            P("dp", "kv", None),
        ),
        out_specs=(P("dp", ("kv", "tp"), None), P("dp", "tp", "kv")),
        check_vma=False,
    )
```
